256 devices in a mesh: ep: 32 (over z, x), tp: 8 (over y, core).
Axes of the slice: x: 4, y: 4, z: 8, core: 2. Of those that a mesh axis runs over, the one named last changes fastest.
Arguments:
- queries: bfloat16 [4096, 4096], P('ep', 'tp'), may hold values from -6 to 6
- key_rows: bfloat16 [4096, 4096], P('ep', 'tp'), may hold values from -6 to 6
- value_rows: bfloat16 [4096, 4096], P('ep', 'tp'), may hold values from -6 to 6
- key_shift: bfloat16 [4096, 64], P('ep', 'tp'), may hold values from -20 to 1
- out_weight: bfloat16 [4096, 4096], P('tp'), may hold values from -0.09375 to 0.09375
- routed_rows: bfloat16 [4096, 4096], P('ep'), may hold values from -6 to 6
- expert_ids: int32 [4096, 2], P('ep'), may hold values from 0 to 31, as said below
- route_weights: float32 [4096, 2], P(('ep', 'tp')), may hold values from 0.2 to 1
- gate_weight: bfloat16 [32, 4096, 1024], P('ep', None, 'tp'), may hold values from -0.09375 to 0.09375
- up_weight: bfloat16 [32, 4096, 1024], P('ep', None, 'tp'), may hold values from -0.09375 to 0.09375
- down_weight: bfloat16 [32, 1024, 4096], P('ep', 'tp'), may hold values from -0.1875 to 0.1875
Outputs:
- mixed_rows: bfloat16 [4096, 4096], P(('ep', 'tp'))
- routed_out: bfloat16 [4096, 4096], P(('ep', 'tp'))
The draws below stay inside these ranges and needn't reach their ends.
Inputs may be any that keep to these rules, and one draw needn't show every extreme that they name: `expert_ids`: the two ids of a token differ and lie in one group of 8 consecutive experts. Within each aligned block of 16 tokens no expert is named more than 2 times.
All inputs are finite; a program needn't handle non-finite values.
Results may differ from the reference program's by a relative error of at most 0.015.
Values may be sent and summed in bfloat16 or wider, within the bound.
No kernel may reach another device: no remote copies, remote signals or barrier semaphores. Data moves between devices by JAX's collectives and lax.ppermute only.
A program may use at most 128 MiB of HBM per device.

```python
import math
import jax
import jax.numpy as jnp
from jax import lax

D = 4096
HEAD_TOTAL = 64
HEAD = 64
FF = 1024
GROUPS = 4
KEY_BLOCK = 512
TOK_EP = 128
SEQUENCE_LENGTH = 4096
EXPERTS = 32
GROUP_SIZE = 8
SUB = 16
CAP = 2
N_TP = 8


def draw_key_shift(key, part):
    quick_key, offset_key, jitter_key, spike_key, level_key = jax.random.split(key, 5)
    fast_share = 0.5
    spike_rate = 2.0 / SEQUENCE_LENGTH
    quick_heads = jax.random.bernoulli(quick_key, fast_share, (HEAD_TOTAL,))
    baseline_level = jnp.where(quick_heads, -6.0, -math.log(SEQUENCE_LENGTH) - 0.5)
    block_start_offset = jnp.repeat(jax.random.uniform(offset_key, (SEQUENCE_LENGTH // TOK_EP, HEAD_TOTAL), jnp.float32, -0.7, 0.7), TOK_EP, axis=0)
    jitter_amount = jax.random.uniform(jitter_key, (SEQUENCE_LENGTH, HEAD_TOTAL), jnp.float32, -0.5, 0.5)
    spike_values = jax.random.bernoulli(spike_key, spike_rate, (SEQUENCE_LENGTH, HEAD_TOTAL)) & jnp.logical_not(quick_heads)[None, :]
    spike_level = jax.random.uniform(level_key, (SEQUENCE_LENGTH, HEAD_TOTAL), jnp.float32, -1.6, -0.7)
    shifted_values = jnp.where(spike_values, spike_level, baseline_level[None, :] + block_start_offset + jitter_amount)
    return shifted_values.astype(jnp.bfloat16)


def draw_expert_ids(key, part):
    full_group = jax.random.randint(jax.random.fold_in(key, 1), (), 0, GROUPS)
    table = jnp.array([[4, 2, 2], [3, 3, 2], [8, 0, 0], [6, 2, 0], [5, 3, 0]], jnp.int32)
    rest = SUB // 2

    def one_block(block_key):
        key_pattern, key_rank, key_order, key_cycle = jax.random.split(block_key, 4)
        pattern = table[jax.random.randint(key_pattern, (), 0, 5)] * (rest // 8)
        ranking = jax.random.permutation(key_rank, GROUPS)
        ranking = jnp.where(jnp.arange(GROUPS, dtype=jnp.int32) == full_group, GROUPS, ranking)
        ordering = jnp.argsort(ranking, stable=True)
        counts = jnp.zeros((GROUPS,), jnp.int32).at[ordering[:GROUPS - 1]].set(pattern)
        counts = counts.at[full_group].set(SUB // 2)
        bounds = jnp.cumsum(counts)
        places = jnp.arange(SUB, dtype=jnp.int32)
        labels = jnp.sum((places[:, None] >= bounds[None, :]).astype(jnp.int32), axis=1)
        within = places - (bounds - counts)[labels]
        shuffle = jax.random.permutation(key_order, SUB)
        labels = labels[shuffle]
        within = within[shuffle]
        cycle_keys = jax.random.split(key_cycle, GROUPS * CAP)
        cycles = jax.vmap(lambda cycle_key: jax.random.permutation(cycle_key, GROUP_SIZE))(cycle_keys)
        cycles = cycles.reshape(GROUPS, CAP, GROUP_SIZE)
        cycle_index = 2 * within // GROUP_SIZE
        place_index = 2 * within % GROUP_SIZE
        first_pick = cycles[labels, cycle_index, place_index]
        second_pick = cycles[labels, cycle_index, place_index + 1]
        return jnp.stack([labels * GROUP_SIZE + first_pick, labels * GROUP_SIZE + second_pick], axis=1).astype(jnp.int32)
    block_keys = jax.random.split(jax.random.fold_in(key, 2), SEQUENCE_LENGTH // SUB)
    return jax.vmap(one_block)(block_keys).reshape(SEQUENCE_LENGTH, 2)


def block_scale(rng, extent, shards, low, largest):
    def one(axis_at, blocks):
        draws = jax.random.uniform(jax.random.fold_in(jax.random.fold_in(rng, 6), axis_at), (blocks,), jnp.float32, low / len(shards), largest / len(shards))
        return jnp.repeat(jnp.exp(draws), extent[axis_at] // blocks).reshape((-1,) + (1,) * (len(extent) - axis_at - 1))

    gain = one(*shards[0])
    for cut in shards[1:]:
        gain = gain * one(*cut)
    return gain


def centred(key, dims, scale, reach, cuts=(), held_as=jnp.bfloat16):
    values = scale * jax.random.normal(key, dims, jnp.float32)
    if cuts:
        values = values * block_scale(key, dims, cuts, -0.22, 0.18)
    return jnp.clip(values, -reach, reach).astype(held_as)


def setup_inputs(seed: int = 0) -> dict:
    keys = jax.random.split(jax.random.key(seed), 12)
    return {
        "queries": centred(keys[0], (SEQUENCE_LENGTH, HEAD_TOTAL * HEAD), 1.0, 6.0, ((0, 32), (1, 8))),
        "key_rows": centred(keys[1], (SEQUENCE_LENGTH, HEAD_TOTAL * HEAD), 1.0, 6.0, ((0, 32), (1, 8))),
        "value_rows": centred(keys[2], (SEQUENCE_LENGTH, HEAD_TOTAL * HEAD), 1.0, 6.0, ((0, 32), (1, 8))),
        "key_shift": draw_key_shift(jax.random.fold_in(keys[11], 71), 0),
        "out_weight": centred(keys[4], (HEAD_TOTAL * HEAD, D), (HEAD_TOTAL * HEAD) ** -0.5, 0.09375, ((0, 8),)),
        "routed_rows": centred(keys[5], (SEQUENCE_LENGTH, D), 1.0, 6.0, ((0, 32),)),
        "expert_ids": draw_expert_ids(jax.random.fold_in(keys[11], 71), 0),
        "route_weights": jnp.clip(0.2 + 0.8 * jax.random.uniform(keys[7], (SEQUENCE_LENGTH, 2), jnp.float32) ** block_scale(keys[7], (SEQUENCE_LENGTH, 2), ((0, 256),), -0.2, 0.2), 0.2, 1.0),
        "gate_weight": centred(keys[8], (EXPERTS, D, FF), D ** -0.5, 0.09375, ((0, 32), (2, 8))),
        "up_weight": centred(keys[9], (EXPERTS, D, FF), D ** -0.5, 0.09375, ((0, 32), (2, 8))),
        "down_weight": centred(keys[10], (EXPERTS, FF, D), FF ** -0.5, 0.1875, ((0, 32), (1, 8))),
    }


def stick_attend(query_rows, key_all, value_all, shift_all, first_pos):
    row_count = query_rows.shape[0]
    head_count = query_rows.shape[1]
    head_depth = query_rows.shape[2]
    query_pos = first_pos + jnp.arange(row_count, dtype=jnp.int32)
    last_block = (first_pos + row_count - 1) // KEY_BLOCK
    score_scale = head_depth ** -0.5
    query_float = query_rows.astype(jnp.float32)

    def sweep_block(step_index, state_pair):
        running, logsum = state_pair
        row_start = ((last_block - step_index) * KEY_BLOCK).astype(jnp.int32)
        key_tile_block = lax.dynamic_slice_in_dim(key_all, row_start, KEY_BLOCK, 0).astype(jnp.float32)
        value_block = lax.dynamic_slice_in_dim(value_all, row_start, KEY_BLOCK, 0).astype(jnp.float32)
        shift_block = lax.dynamic_slice_in_dim(shift_all, row_start, KEY_BLOCK, 0).astype(jnp.float32)
        scores = jnp.einsum("thd,shd->hts", query_float, key_tile_block) * score_scale + shift_block.T[:, None, :]
        key_pos = row_start + jnp.arange(KEY_BLOCK, dtype=jnp.int32)
        strict = (key_pos[None, :] < query_pos[:, None])[None]
        log_keep = jnp.where(strict, jax.nn.log_sigmoid(-scores), 0.0)
        suffix = lax.cumsum(log_keep, axis=2, reverse=True) - log_keep + logsum[:, :, None]
        weight = jnp.where(strict, jnp.exp(jax.nn.log_sigmoid(scores) + suffix), 0.0).astype(jnp.bfloat16)
        running = running + jnp.einsum("hts,shd->htd", weight.astype(jnp.float32), value_block)
        return running, logsum + jnp.sum(log_keep, axis=2)

    initial = (jnp.zeros((head_count, row_count, head_depth), jnp.float32),
               jnp.zeros((head_count, row_count), jnp.float32))
    running, logsum = lax.fori_loop(0, last_block + 1, sweep_block, initial)
    return jnp.transpose(running, (1, 0, 2)).reshape(row_count, head_count * head_depth).astype(jnp.bfloat16)


def slot_numbers(pair_ids, expert_count):
    one_hot = (pair_ids[..., None] == jnp.arange(expert_count, dtype=jnp.int32)).astype(jnp.int32)
    earlier = jnp.cumsum(one_hot, axis=1) - one_hot
    return jnp.sum(one_hot * earlier, axis=2)


def reference(queries, key_rows, value_rows, key_shift, out_weight, routed_rows, expert_ids,
              route_weights, gate_weight, up_weight, down_weight):
    query_heads = queries.reshape(SEQUENCE_LENGTH, HEAD_TOTAL, HEAD)
    key_heads = key_rows.reshape(SEQUENCE_LENGTH, HEAD_TOTAL, HEAD)
    value_heads = value_rows.reshape(SEQUENCE_LENGTH, HEAD_TOTAL, HEAD)
    block_count = SEQUENCE_LENGTH // KEY_BLOCK

    def one_block(pair):
        query_block, block_index = pair
        return stick_attend(query_block, key_heads, value_heads, key_shift, block_index * KEY_BLOCK)

    attended = lax.map(one_block, (query_heads.reshape(block_count, KEY_BLOCK, HEAD_TOTAL, HEAD),
                                   jnp.arange(block_count, dtype=jnp.int32)))
    attended = attended.reshape(SEQUENCE_LENGTH, HEAD_TOTAL * HEAD)
    group_cols = HEAD_TOTAL * HEAD // N_TP
    mixed_sum = jnp.zeros((SEQUENCE_LENGTH, D), jnp.float32)
    for group in range(N_TP):
        partial_value = jnp.dot(attended[:, group * group_cols:(group + 1) * group_cols],
                          out_weight[group * group_cols:(group + 1) * group_cols],
                          preferred_element_type=jnp.float32).astype(jnp.bfloat16)
        partial_value = lax.optimization_barrier(partial_value)
        mixed_sum = mixed_sum + partial_value.astype(jnp.float32)
    mixed_rows = mixed_sum.astype(jnp.bfloat16)

    sub_count = SEQUENCE_LENGTH // SUB
    pair_ids = expert_ids.reshape(sub_count, SUB * 2)
    slots = slot_numbers(pair_ids, EXPERTS)
    block_ids = jnp.arange(sub_count, dtype=jnp.int32)[:, None]
    position = (block_ids * CAP + slots).reshape(-1)
    flat_ids = pair_ids.reshape(-1)
    token_index = jnp.arange(SEQUENCE_LENGTH * 2, dtype=jnp.int32) // 2
    dispatched = jnp.zeros((EXPERTS, sub_count * CAP, D), jnp.bfloat16)
    dispatched = dispatched.at[flat_ids, position].set(routed_rows[token_index])
    unit_group = FF // N_TP

    def one_expert(operands):
        expert_rows, gate_part, up_part, down_part = operands
        gate_proj = jnp.dot(expert_rows, gate_part, preferred_element_type=jnp.float32)
        up_proj = jnp.dot(expert_rows, up_part, preferred_element_type=jnp.float32)
        hidden = (jax.nn.silu(gate_proj) * up_proj).astype(jnp.bfloat16)
        summed = jnp.zeros((expert_rows.shape[0], D), jnp.float32)
        for group in range(N_TP):
            partial_value = jnp.dot(hidden[:, group * unit_group:(group + 1) * unit_group],
                              down_part[group * unit_group:(group + 1) * unit_group],
                              preferred_element_type=jnp.float32).astype(jnp.bfloat16)
            partial_value = lax.optimization_barrier(partial_value)
            summed = summed + partial_value.astype(jnp.float32)
        return summed.astype(jnp.bfloat16)

    expert_out = lax.map(one_expert, (dispatched, gate_weight, up_weight, down_weight))
    picked = expert_out[flat_ids, position].reshape(SEQUENCE_LENGTH, 2, D).astype(jnp.float32)
    routed_out = (picked[:, 0] * route_weights[:, 0:1] + picked[:, 1] * route_weights[:, 1:2]).astype(jnp.bfloat16)
    return mixed_rows, routed_out
```

```python
import jax
import jax.numpy as jnp
from jax import lax
from jax.experimental import pallas as pl
from jax.experimental.pallas import tpu as pltpu
from jax.sharding import Mesh, PartitionSpec as P

HEAD = 64
Z, X, Y, C = 8, 4, 4, 2
BF = jnp.bfloat16
F32 = jnp.float32

STEPS = (
    ((7, 6), (6, 5), (5, 4), (4, 3)),
    ((7, 5), (6, 4), (5, 3), (4, 2)),
    ((7, 4), (6, 3), (5, 2), (4, 1)),
    ((7, 3), (6, 2), (5, 1), (4, 0)),
    ((7, 2), (6, 1), (5, 0), (3, 2)),
    ((7, 1), (6, 0), (3, 1), (2, 1)),
    ((7, 0), (3, 0), (2, 0), (1, 0)),
)


def attend_kernel(x_ref, steps_ref, q_ref, k0_ref, k1_ref, k2_ref, k3_ref, o_ref, kv_ref, qs_ref, tri_ref, carry_ref, acc_ref):
    here = x_ref[0]
    for shift, piece in enumerate((k0_ref, k1_ref, k2_ref, k3_ref)):
        kv_ref[lax.rem(here + (4 - shift), 4)] = piece[...]
    row = lax.broadcasted_iota(jnp.int32, (256, 256), 0)
    col = lax.broadcasted_iota(jnp.int32, (256, 256), 1)
    tri = jnp.where(row > col, 1.0, 0.0).astype(BF)
    tri_ref[0:256] = tri
    tri_ref[256:512] = tri
    ones = jnp.where(lax.broadcasted_iota(jnp.int32, (64, 128), 0) == 0, 1.0, 0.0)
    for b in range(8):
        q = jnp.concatenate([q_ref[b].astype(F32), ones], axis=0)
        qs_ref[b] = jnp.transpose(q).astype(BF)

    def scores(b, t):
        keys = jnp.concatenate([kv_ref[i, t, 0:80, :] for i in range(4)], axis=1)
        return jnp.dot(qs_ref[b][:, 0:80], keys, preferred_element_type=F32)

    def tile(b, t, mask, carry):
        s = scores(b, t)
        sp = jnp.maximum(s, jnp.log(1.0 + jnp.exp(jnp.minimum(s, 80.0))))
        if mask is not None:
            sp = jnp.where(mask, sp, 0.0)
        high = sp.astype(BF)
        low = (sp - high.astype(F32)).astype(BF)
        logit = s - sp
        weights = [None, None]
        for half in (1, 0):
            at = slice(half * 256, half * 256 + 256)
            after = jnp.dot(
                jnp.concatenate([high[:, at], low[:, at]], axis=1), tri_ref[...], preferred_element_type=F32
            )
            w = jnp.exp(logit[:, at] - after - carry)
            if mask is not None:
                w = jnp.where(mask[:, at], w, 0.0)
            weights[half] = w.astype(BF)
            carry = carry + after[:, 0:1] + sp[:, half * 256 : half * 256 + 1]
        values = jnp.concatenate([kv_ref[i, t, 80:144, :] for i in range(4)], axis=1)
        out = lax.dot_general(
            jnp.concatenate(weights, axis=1), values, (((1,), (1,)), ((), ())), preferred_element_type=F32
        )
        return out, carry

    def diagonal(i, unused):
        q_at = here * 128 + lax.broadcasted_iota(jnp.int32, (128, 512), 0)
        mask = lax.broadcasted_iota(jnp.int32, (128, 512), 1) < q_at
        done = [tile(i * 4 + j, i * 4 + j, mask, jnp.zeros((128, 1), F32)) for j in range(4)]
        for j in range(4):
            acc_ref[i * 4 + j] = done[j][0]
            carry_ref[i * 4 + j] = done[j][1]
        return unused

    lax.fori_loop(0, 2, diagonal, 0)

    def sweep(i, unused):
        blocks = [steps_ref[i, 2 * j] for j in range(4)]
        tiles = [steps_ref[i, 2 * j + 1] for j in range(4)]
        carries = [carry_ref[b] for b in blocks]
        before = [acc_ref[b] for b in blocks]
        done = [tile(blocks[j], tiles[j], None, carries[j]) for j in range(4)]
        for j in range(4):
            acc_ref[blocks[j]] = before[j] + done[j][0]
            carry_ref[blocks[j]] = done[j][1]
        return unused

    lax.fori_loop(0, len(STEPS), sweep, 0)
    for b in range(8):
        o_ref[b] = jnp.transpose(acc_ref[b]).astype(BF)


def attend(q, pieces, x):
    vmem = pl.BlockSpec(memory_space=pltpu.VMEM)
    smem = pl.BlockSpec(memory_space=pltpu.SMEM)
    steps = jnp.array([[v for pair in step for v in pair] for step in STEPS], jnp.int32)
    return pl.pallas_call(
        attend_kernel,
        out_shape=jax.ShapeDtypeStruct((8, HEAD, 128), BF),
        in_specs=[smem, smem] + [vmem] * 5,
        out_specs=vmem,
        scratch_shapes=[
            pltpu.VMEM((4, 8, 144, 128), BF),
            pltpu.VMEM((8, 128, 128), BF),
            pltpu.VMEM((512, 256), BF),
            pltpu.VMEM((8, 128, 1), F32),
            pltpu.VMEM((8, 128, HEAD), F32),
        ],
        compiler_params=pltpu.CompilerParams(vmem_limit_bytes=32 * 1024 * 1024),
        cost_estimate=pl.CostEstimate(flops=4_000_000_000, transcendentals=7_000_000, bytes_accessed=2_000_000),
    )(x.reshape(1), steps, q, *pieces)


def shifted(value, axis, size, by):
    return lax.ppermute(value, axis, [(i, (i + by) % size) for i in range(size)])


def mixer(queries, key_rows, value_rows, key_shift, out_weight):
    heads = key_shift.shape[1]
    rows = queries.shape[0]
    x = lax.axis_index("x")

    def by_head(a):
        return a.T.reshape(heads, HEAD, rows)

    packed = jnp.concatenate(
        [
            by_head(queries * jnp.asarray(HEAD**-0.5, BF)),
            by_head(key_rows),
            jnp.pad(key_shift.T[:, None, :], ((0, 0), (0, 15), (0, 0))),
            by_head(value_rows),
        ],
        axis=1,
    )
    arrived = lax.all_to_all(packed, "z", split_axis=0, concat_axis=0, tiled=True)
    keys = arrived[:, HEAD:, :]
    pieces = [keys] + [shifted(keys, "x", X, by) for by in (1, 2, 3)]
    out = attend(arrived[:, :HEAD, :], pieces, x)
    attended = lax.all_to_all(out, "z", split_axis=0, concat_axis=0, tiled=True).reshape(heads * HEAD, rows)
    partial = lax.dot_general(attended, out_weight, (((0,), (0,)), ((), ())), preferred_element_type=F32)
    return summed_over_tp(partial)


def summed_over_tp(partial):
    y, core = lax.axis_index("y"), lax.axis_index("c")
    rows, width = partial.shape
    per = rows // (Y * C)
    parts = partial.astype(BF).reshape(Y, C, per, width)
    mine = lax.dynamic_index_in_dim(parts, core, 1, keepdims=False)
    other = lax.dynamic_index_in_dim(parts, 1 - core, 1, keepdims=False)
    both = (mine.astype(F32) + shifted(other, "c", C, 1).astype(F32)).astype(BF)
    total = lax.dynamic_index_in_dim(both, y, 0, keepdims=False).astype(F32)
    for by in (1, 2, 3):
        piece = lax.dynamic_index_in_dim(both, lax.rem(y + by, Y), 0, keepdims=False)
        total = total + shifted(piece, "y", Y, by).astype(F32)
    return total.astype(BF)


def in_blocks(value, dim, peers):
    before, after = (value.shape[:dim], value.shape[dim + 1 :])
    return jnp.moveaxis(value.reshape(*before, peers, -1, *after), dim, 0)


def sent_and_summed(value, axis, peers):
    tiles = in_blocks(value, 0, peers)
    arrived = lax.all_to_all(tiles, axis, split_axis=0, concat_axis=0, tiled=True)
    return arrived.astype(jnp.float32).sum(axis=0)


def slot_numbers(pair_ids, expert_count):
    one_hot = (pair_ids[..., None] == jnp.arange(expert_count, dtype=jnp.int32)).astype(jnp.int32)
    earlier = jnp.cumsum(one_hot, axis=1) - one_hot
    return jnp.sum(one_hot * earlier, axis=2)


def pack_rows(source_rows, destination, slot_count):
    pair_count = destination.shape[0]
    matches = destination[None, :] == jnp.arange(slot_count, dtype=jnp.int32)[:, None]
    source_index = jnp.sum(
        jnp.where(matches, jnp.arange(pair_count, dtype=jnp.int32)[None, :] // 2, 0), axis=1
    )
    filled = jnp.any(matches, axis=1)
    picked = jnp.take(source_rows, source_index, axis=0)
    return jnp.where(filled[:, None], picked, jnp.zeros_like(picked))


def expand(expert_rows, gate_part, up_part):
    gate_proj = jnp.einsum(
        "rcd,df->rcf", expert_rows, gate_part, preferred_element_type=jnp.float32
    )
    up_proj = jnp.einsum("rcd,df->rcf", expert_rows, up_part, preferred_element_type=jnp.float32)
    return (jax.nn.silu(gate_proj) * up_proj).astype(jnp.bfloat16)


def experts(routed_rows, expert_ids, route_weights, gate_weight, up_weight, down_weight):
    ep, tp = ("z", "x"), ("y", "c")
    tp_count = Y * C
    local_rows = routed_rows.shape[0]
    expert_count = Z * X
    sub_rows = local_rows // tp_count
    capacity = 4 * sub_rows // expert_count
    model_width = routed_rows.shape[1]
    column = lax.axis_index("y") * C + lax.axis_index("c")
    own_ids = lax.dynamic_slice_in_dim(expert_ids, column * sub_rows, sub_rows, 0).reshape(
        1, sub_rows * 2
    )
    own_slot = slot_numbers(own_ids, expert_count)[0]
    own_dest = own_ids[0] * capacity + own_slot
    own_input = lax.dynamic_slice_in_dim(routed_rows, column * sub_rows, sub_rows, 0)
    outgoing = pack_rows(own_input, own_dest, expert_count * capacity).reshape(
        expert_count, capacity, model_width
    )
    arrived = lax.all_to_all(outgoing, ep, split_axis=0, concat_axis=0, tiled=True)
    hidden = expand(lax.all_gather(arrived, tp, axis=1, tiled=True), gate_weight[0], up_weight[0])
    unit_count = hidden.shape[2]
    ordered = jnp.transpose(
        hidden.reshape(expert_count, tp_count, capacity, unit_count), (1, 0, 2, 3)
    )
    ordered = ordered.reshape(tp_count * expert_count * capacity, unit_count)
    partial_value = sent_and_summed(
        jnp.dot(ordered, down_weight[0], preferred_element_type=jnp.float32).astype(jnp.bfloat16),
        tp,
        tp_count,
    ).astype(jnp.bfloat16)
    returned = lax.all_to_all(
        partial_value.reshape(expert_count, capacity, model_width),
        ep,
        split_axis=0,
        concat_axis=0,
        tiled=True,
    )
    picked = jnp.take(returned.reshape(expert_count * capacity, model_width), own_dest, axis=0)
    picked = picked.reshape(sub_rows, 2, model_width).astype(jnp.float32)
    return (
        picked[:, 0] * route_weights[:, 0:1] + picked[:, 1] * route_weights[:, 1:2]
    ).astype(jnp.bfloat16)


def shards(
    queries,
    key_rows,
    value_rows,
    key_shift,
    out_weight,
    routed_rows,
    expert_ids,
    route_weights,
    gate_weight,
    up_weight,
    down_weight,
):
    mixed_rows = mixer(queries, key_rows, value_rows, key_shift, out_weight)
    routed_out = experts(routed_rows, expert_ids, route_weights, gate_weight, up_weight, down_weight)
    return (mixed_rows, routed_out)


def solution(mesh):
    mesh = Mesh(mesh.devices.reshape(Z, X, Y, C), ("z", "x", "y", "c"))
    ep, tp = ("z", "x"), ("y", "c")
    return jax.shard_map(
        shards,
        mesh=mesh,
        in_specs=(
            P(ep, tp),
            P(ep, tp),
            P(ep, tp),
            P(ep, tp),
            P(tp, None),
            P(ep, None),
            P(ep, None),
            P(ep + tp, None),
            P(ep, None, tp),
            P(ep, None, tp),
            P(ep, tp, None),
        ),
        out_specs=(P(ep + tp, None), P(ep + tp, None)),
        check_vma=False,
    )
```

```python
import jax
import jax.numpy as jnp
from jax import lax
from jax.experimental import pallas as pl
from jax.experimental.pallas import tpu as pltpu
from jax.sharding import Mesh, PartitionSpec as P


HEAD = 64
Z, X, Y, C = 8, 4, 4, 2
BF = jnp.bfloat16
F32 = jnp.float32

STEPS = (
    ((7, 6), (6, 5), (5, 4), (4, 3)),
    ((7, 5), (6, 4), (5, 3), (4, 2)),
    ((7, 4), (6, 3), (5, 2), (4, 1)),
    ((7, 3), (6, 2), (5, 1), (4, 0)),
    ((7, 2), (6, 1), (5, 0), (3, 2)),
    ((7, 1), (6, 0), (3, 1), (2, 1)),
    ((7, 0), (3, 0), (2, 0), (1, 0)),
)


def attend_kernel(*refs):
    arrived, (k1_ref, k2_ref, k3_ref, o_ref) = refs[:Z], refs[Z : Z + 4]
    attend_body(arrived, k1_ref, k2_ref, k3_ref, o_ref, *refs[Z + 4 :])


def attend_body(arrived, k1_ref, k2_ref, k3_ref, o_ref, kv_ref, qs_ref, tri_ref, carry_ref, acc_ref, steps_ref):
    here = lax.axis_index("x")
    plane = lax.axis_index("z")
    for i in range(Z):
        at = lax.rem(plane + (Z - i), Z)
        kv_ref[here, at] = arrived[i][HEAD:]
        for shift, piece in ((1, k1_ref), (2, k2_ref), (3, k3_ref)):
            kv_ref[lax.rem(here + (X - shift), X), at] = piece[i]
    row = lax.broadcasted_iota(jnp.int32, (256, 256), 0)
    col = lax.broadcasted_iota(jnp.int32, (256, 256), 1)
    tri = jnp.where(row > col, 1.0, 0.0).astype(BF)
    tri_ref[0:256] = tri
    tri_ref[256:512] = tri
    ones = jnp.where(lax.broadcasted_iota(jnp.int32, (64, 128), 0) == 0, 1.0, 0.0)
    for i in range(Z):
        q = jnp.concatenate([arrived[i][:HEAD].astype(F32), ones], axis=0)
        qs_ref[lax.rem(plane + (Z - i), Z)] = jnp.transpose(q).astype(BF)
    for i, step in enumerate(STEPS):
        for j, pair in enumerate(step):
            steps_ref[i, 2 * j] = pair[0]
            steps_ref[i, 2 * j + 1] = pair[1]

    def scores(b, t):
        keys = jnp.concatenate([kv_ref[i, t, 0:80, :] for i in range(4)], axis=1)
        return jnp.dot(qs_ref[b][:, 0:80], keys, preferred_element_type=F32)

    def tile(b, t, mask, carry):
        s = scores(b, t)
        sp = jnp.maximum(s, jnp.log(1.0 + jnp.exp(jnp.minimum(s, 80.0))))
        if mask is not None:
            sp = jnp.where(mask, sp, 0.0)
        high = sp.astype(BF)
        low = (sp - high.astype(F32)).astype(BF)
        logit = s - sp
        weights = [None, None]
        for half in (1, 0):
            at = slice(half * 256, half * 256 + 256)
            after = jnp.dot(
                jnp.concatenate([high[:, at], low[:, at]], axis=1), tri_ref[...], preferred_element_type=F32
            )
            w = jnp.exp(logit[:, at] - after - carry)
            if mask is not None:
                w = jnp.where(mask[:, at], w, 0.0)
            weights[half] = w.astype(BF)
            carry = carry + after[:, 0:1] + sp[:, half * 256 : half * 256 + 1]
        values = jnp.concatenate([kv_ref[i, t, 80:144, :] for i in range(4)], axis=1)
        out = lax.dot_general(
            jnp.concatenate(weights, axis=1), values, (((1,), (1,)), ((), ())), preferred_element_type=F32
        )
        return out, carry

    def diagonal(i, unused):
        q_at = here * 128 + lax.broadcasted_iota(jnp.int32, (128, 512), 0)
        mask = lax.broadcasted_iota(jnp.int32, (128, 512), 1) < q_at
        done = [tile(i * 4 + j, i * 4 + j, mask, jnp.zeros((128, 1), F32)) for j in range(4)]
        for j in range(4):
            acc_ref[i * 4 + j] = done[j][0]
            carry_ref[i * 4 + j] = done[j][1]
        return unused

    lax.fori_loop(0, 2, diagonal, 0)

    def sweep(i, unused):
        blocks = [steps_ref[i, 2 * j] for j in range(4)]
        tiles = [steps_ref[i, 2 * j + 1] for j in range(4)]
        carries = [carry_ref[b] for b in blocks]
        before = [acc_ref[b] for b in blocks]
        done = [tile(blocks[j], tiles[j], None, carries[j]) for j in range(4)]
        for j in range(4):
            acc_ref[blocks[j]] = before[j] + done[j][0]
            carry_ref[blocks[j]] = done[j][1]
        return unused

    lax.fori_loop(0, len(STEPS), sweep, 0)
    for b in range(8):
        o_ref[b] = jnp.transpose(acc_ref[b]).astype(BF)


VMEM = pl.BlockSpec(memory_space=pltpu.VMEM)
ANY = pl.BlockSpec(memory_space=pl.ANY)


def attend(arrived, pieces):
    return pl.pallas_call(
        attend_kernel,
        out_shape=jax.ShapeDtypeStruct((8, HEAD, 128), BF),
        in_specs=[VMEM] * (Z + 3),
        out_specs=VMEM,
        scratch_shapes=[
            pltpu.VMEM((4, 8, 144, 128), BF),
            pltpu.VMEM((8, 128, 128), BF),
            pltpu.VMEM((512, 256), BF),
            pltpu.VMEM((8, 128, 1), F32),
            pltpu.VMEM((8, 128, HEAD), F32),
            pltpu.SMEM((len(STEPS), 8), jnp.int32),
        ],
        compiler_params=pltpu.CompilerParams(vmem_limit_bytes=32 * 1024 * 1024),
        cost_estimate=pl.CostEstimate(flops=4_000_000_000, transcendentals=7_000_000, bytes_accessed=2_000_000),
    )(*arrived, *pieces)


def pack_kernel(q_ref, k_ref, v_ref, shift_ref, *refs):
    outs, (q_all, k_all, v_all, shift_all) = refs[:Z], refs[Z:]
    plane = lax.axis_index("z")
    q_all[...] = jnp.transpose(q_ref[...].astype(F32) * HEAD**-0.5)
    k_all[...] = jnp.transpose(k_ref[...].astype(F32))
    v_all[...] = jnp.transpose(v_ref[...].astype(F32))
    shift_all[...] = shift_ref[...].astype(F32)
    first = lax.broadcasted_iota(jnp.int32, (16, 128), 0) == 0
    for s, out in enumerate(outs):
        head = lax.rem(plane + s, Z)
        rows = pl.ds(pl.multiple_of(head * HEAD, HEAD), HEAD)
        out[0:64] = q_all[rows, :].astype(BF)
        out[64:128] = k_all[rows, :].astype(BF)
        shift = jnp.broadcast_to(shift_all[pl.ds(head, 1), :], (16, 128))
        out[128:144] = jnp.where(first, shift, 0.0).astype(BF)
        out[144:208] = v_all[rows, :].astype(BF)


def stack_kernel(*refs):
    for i in range(Z):
        refs[Z][i] = refs[i][HEAD:]


def stacked(arrived):
    return pl.pallas_call(
        stack_kernel,
        out_shape=jax.ShapeDtypeStruct((Z, 144, 128), BF),
        in_specs=[VMEM] * Z,
        out_specs=VMEM,
    )(*arrived)


def pack(queries, key_rows, value_rows, shift):
    rows, width = queries.shape
    return pl.pallas_call(
        pack_kernel,
        out_shape=[jax.ShapeDtypeStruct((208, 128), BF)] * Z,
        in_specs=[VMEM] * 4,
        out_specs=[VMEM] * Z,
        scratch_shapes=[pltpu.VMEM((width, rows), F32)] * 3 + [pltpu.VMEM((8, rows), F32)],
    )(queries, key_rows, value_rows, shift)


def shifted(value, axis, size, by):
    return lax.ppermute(value, axis, [(i, (i + by) % size) for i in range(size)])


def mixer(queries, key_rows, value_rows, key_shift, out_weight):
    heads = key_shift.shape[1]
    rows = queries.shape[0]
    packed = pack(queries, key_rows, value_rows, key_shift.T)
    arrived = [packed[0]] + [shifted(packed[by], "z", Z, by) for by in range(1, Z)]
    keys = stacked(arrived)
    pieces = [shifted(keys, "x", X, by) for by in (1, 2, 3)]
    out = attend(arrived, pieces)
    attended = lax.all_to_all(out, "z", split_axis=0, concat_axis=0, tiled=True)
    attended = attended.reshape(heads * HEAD, rows)
    partial = lax.dot_general(
        attended, out_weight, (((0,), (0,)), ((), ())), preferred_element_type=F32
    ).astype(BF)
    return summed_over_tp(partial)


def summed_over_tp(partial):
    y, core = lax.axis_index("y"), lax.axis_index("c")
    rows, width = partial.shape
    per = rows // (Y * C)
    parts = partial.reshape(Y, C, per, width)
    mine = lax.dynamic_index_in_dim(parts, core, 1, keepdims=False)
    other = lax.dynamic_index_in_dim(parts, 1 - core, 1, keepdims=False)
    both = (mine.astype(F32) + shifted(other, "c", C, 1).astype(F32)).astype(BF)
    total = lax.dynamic_index_in_dim(both, y, 0, keepdims=False).astype(F32)
    for by in (1, 2, 3):
        piece = lax.dynamic_index_in_dim(both, lax.rem(y + by, Y), 0, keepdims=False)
        total = total + shifted(piece, "y", Y, by).astype(F32)
    return total.astype(BF)


def selection(ids_ref, core):
    row = lax.broadcasted_iota(jnp.int32, (256, 128), 0)
    token = lax.broadcasted_iota(jnp.int32, (256, 128), 1)
    expert = lax.div(row, 8)
    named = [ids_ref[k : k + 1, :] == expert for k in range(2)]
    either = jnp.where(named[0] | named[1], 1.0, 0.0)
    before = lax.broadcasted_iota(jnp.int32, (128, 128), 0)
    after = lax.broadcasted_iota(jnp.int32, (128, 128), 1)
    earlier = jnp.where((before < after) & (lax.div(before, 16) == lax.div(after, 16)), 1.0, 0.0)
    slot = jnp.dot(either.astype(BF), earlier.astype(BF), preferred_element_type=F32)
    here = (lax.div(token, 16) == 2 * lax.div(lax.rem(row, 8), 2) + core) & (
        slot == lax.rem(row, 2).astype(F32)
    )
    return [jnp.where(n & here, 1.0, 0.0) for n in named]


def dispatch_kernel(ids_ref, rows_ref, out_ref, part_ref, sem):
    width = out_ref.shape[1]
    start = pl.multiple_of(lax.axis_index("y") * width, width)
    copy = pltpu.make_async_copy(rows_ref.at[:, pl.ds(start, width)], part_ref, sem)
    copy.start()
    first, second = selection(ids_ref, lax.axis_index("c"))
    pick = (first + second).astype(BF)
    copy.wait()
    out_ref[...] = jnp.dot(pick, part_ref[...], preferred_element_type=F32).astype(BF)


def dispatch(ids, rows):
    width = rows.shape[1] // Y
    return pl.pallas_call(
        dispatch_kernel,
        out_shape=jax.ShapeDtypeStruct((256, width), BF),
        in_specs=[VMEM, ANY],
        out_specs=VMEM,
        scratch_shapes=[pltpu.VMEM((128, width), BF), pltpu.SemaphoreType.DMA],
    )(ids, rows)


def collect_kernel(ids_ref, rows_ref, o0_ref, o1_ref, o2_ref, o3_ref, all_ref):
    y, core = lax.axis_index("y"), lax.axis_index("c")
    for k, pick in enumerate(selection(ids_ref, core)):
        chosen = jnp.transpose(pick).astype(BF)
        all_ref[k] = jnp.dot(chosen, rows_ref[...], preferred_element_type=F32).astype(BF)
        for s, out in enumerate((o0_ref, o1_ref, o2_ref, o3_ref)):
            at = pl.multiple_of((2 * lax.rem(y + s, Y) + core) * 16, 16)
            out[k] = all_ref[k, pl.ds(at, 16), :]


def collect(ids, rows):
    width = rows.shape[1]
    return pl.pallas_call(
        collect_kernel,
        out_shape=[jax.ShapeDtypeStruct((2, 16, width), BF)] * Y,
        in_specs=[VMEM, VMEM],
        out_specs=[VMEM] * Y,
        scratch_shapes=[pltpu.VMEM((2, 128, width), BF)],
    )(ids, rows)


def finish_kernel(p0_ref, p1_ref, p2_ref, p3_ref, weights_ref, out_ref):
    w = weights_ref[...]
    width = p0_ref.shape[2]
    for s, p in enumerate((p0_ref, p1_ref, p2_ref, p3_ref)):
        at = pl.multiple_of(lax.rem(lax.axis_index("y") + (Y - s), Y) * width, width)
        total = p[0].astype(F32) * w[:, 0:1] + p[1].astype(F32) * w[:, 1:2]
        out_ref[:, pl.ds(at, width)] = total.astype(BF)


def finish(picked, weights):
    return pl.pallas_call(
        finish_kernel,
        out_shape=jax.ShapeDtypeStruct((16, Y * picked[0].shape[2]), BF),
        in_specs=[VMEM] * 5,
        out_specs=VMEM,
    )(*picked, weights)


def share_kernel(gate_ref, up_ref, down_ref, o1_ref, o2_ref, o3_ref, sem):
    width = gate_ref.shape[0] // Y
    copies = []
    for s, out in ((1, o1_ref), (2, o2_ref), (3, o3_ref)):
        start = pl.multiple_of(lax.rem(lax.axis_index("y") + s, Y) * width, width)
        copies.append((gate_ref.at[pl.ds(start, width), :], out.at[pl.ds(0, width), :]))
        copies.append((up_ref.at[pl.ds(start, width), :], out.at[pl.ds(width, width), :]))
        for j in range(width // 128):
            copies.append(
                (
                    down_ref.at[:, pl.ds(pl.multiple_of(start + j * 128, 128), 128)],
                    out.at[pl.ds(2 * width + j * 128, 128), :],
                )
            )
    made = [pltpu.make_async_copy(a, b, sem.at[n]) for n, (a, b) in enumerate(copies)]
    for m in made:
        m.start()
    for m in made:
        m.wait()


def share(gate, up, down):
    width = gate.shape[0] // Y
    out = jax.ShapeDtypeStruct((3 * width, 128), BF)
    return pl.pallas_call(
        share_kernel,
        out_shape=[out] * (Y - 1),
        in_specs=[ANY, ANY, ANY],
        out_specs=[VMEM] * (Y - 1),
        scratch_shapes=[pltpu.SemaphoreType.DMA(((Y - 1) * (2 + width // 128),))],
    )(gate, up, down)


def expand_kernel(
    own_ref, other_ref, gate_ref, up_ref, w1_ref, w2_ref, w3_ref, o0_ref, o1_ref, o2_ref, o3_ref, kept_ref, sem
):
    width = own_ref.shape[1]
    rows = own_ref.shape[0]
    start = pl.multiple_of(lax.axis_index("y") * width, width)
    copies = [
        pltpu.make_async_copy(ref.at[pl.ds(start, width), :], kept_ref.at[n], sem.at[n])
        for n, ref in enumerate((gate_ref, up_ref))
    ]
    for copy in copies:
        copy.start()

    def into(o_ref, w):
        o_ref[0:rows] = jnp.dot(own_ref[...], w, preferred_element_type=F32).astype(o_ref.dtype)
        o_ref[rows : 2 * rows] = jnp.dot(other_ref[...], w, preferred_element_type=F32).astype(o_ref.dtype)

    for w_ref, o_ref in ((w1_ref, o1_ref), (w2_ref, o2_ref), (w3_ref, o3_ref)):
        into(o_ref, jnp.concatenate([w_ref[0:width], w_ref[width : 2 * width]], axis=1))
    for copy in copies:
        copy.wait()
    into(o0_ref, jnp.concatenate([kept_ref[0], kept_ref[1]], axis=1))


def expand(own, other, gate, up, shared):
    rows = 2 * own.shape[0]
    width = own.shape[1]
    sent = jax.ShapeDtypeStruct((rows, 256), BF)
    return pl.pallas_call(
        expand_kernel,
        out_shape=[jax.ShapeDtypeStruct((rows, 256), F32), sent, sent, sent],
        in_specs=[VMEM, VMEM, ANY, ANY] + [VMEM] * 3,
        out_specs=[VMEM] * 4,
        scratch_shapes=[pltpu.VMEM((2, width, 128), BF), pltpu.SemaphoreType.DMA((2,))],
        compiler_params=pltpu.CompilerParams(vmem_limit_bytes=32 * 1024 * 1024),
    )(own, other, gate, up, *shared)


def hidden_kernel(p0_ref, p1_ref, p2_ref, p3_ref, o_ref):
    both = p0_ref[...]
    for p in (p1_ref, p2_ref, p3_ref):
        both = both + p[...].astype(F32)
    gate, up = both[:, 0:128], both[:, 128:256]
    o_ref[...] = (gate / (1.0 + jnp.exp(-gate)) * up).astype(BF)


def hidden_units(parts):
    return pl.pallas_call(
        hidden_kernel,
        out_shape=jax.ShapeDtypeStruct((parts[0].shape[0], 128), BF),
        in_specs=[VMEM] * 4,
        out_specs=VMEM,
    )(*parts)


def reduce_kernel(
    h0_ref, h1_ref, h2_ref, h3_ref, down_ref, w1_ref, w2_ref, w3_ref, own_ref, other_ref, kept_ref, sem
):
    rows, width = own_ref.shape
    start = pl.multiple_of(lax.axis_index("y") * width, width)
    copy = pltpu.make_async_copy(down_ref.at[:, pl.ds(start, width)], kept_ref, sem)
    copy.start()
    units = jnp.concatenate([h[...] for h in (h1_ref, h2_ref, h3_ref, h0_ref)], axis=1)
    columns = []
    for w_ref in (w1_ref, w2_ref, w3_ref):
        blocks = [w_ref[2 * width + j * 128 : 2 * width + j * 128 + 128] for j in range(width // 128)]
        columns.append(jnp.concatenate(blocks, axis=1))
    copy.wait()
    w = jnp.concatenate(columns + [kept_ref[...]], axis=0)
    other_ref[...] = jnp.dot(units[rows:], w, preferred_element_type=F32).astype(BF)
    own_ref[...] = jnp.dot(units[:rows], w, preferred_element_type=F32)


def reduce_units(units, down, shared):
    rows = units[0].shape[0] // 2
    width = shared[0].shape[0] // 3
    return pl.pallas_call(
        reduce_kernel,
        out_shape=[jax.ShapeDtypeStruct((rows, width), F32), jax.ShapeDtypeStruct((rows, width), BF)],
        in_specs=[VMEM] * 4 + [ANY] + [VMEM] * 3,
        out_specs=[VMEM] * 2,
        scratch_shapes=[pltpu.VMEM((128, width), BF), pltpu.SemaphoreType.DMA],
        compiler_params=pltpu.CompilerParams(vmem_limit_bytes=32 * 1024 * 1024),
    )(*units, down, *shared)


def add_kernel(a_ref, b_ref, o_ref):
    o_ref[...] = (a_ref[...] + b_ref[...].astype(F32)).astype(BF)


def added(a, b):
    return pl.pallas_call(
        add_kernel,
        out_shape=jax.ShapeDtypeStruct(a.shape, BF),
        in_specs=[VMEM, VMEM],
        out_specs=VMEM,
    )(a, b)


def experts(routed_rows, expert_ids, route_weights, gate_weight, up_weight, down_weight):
    ep = ("z", "x")
    ids = expert_ids.T
    width = routed_rows.shape[1] // Y
    kept = share(gate_weight[0], up_weight[0], down_weight[0])
    shared = [shifted(kept[s - 1], "y", Y, s) for s in (1, 2, 3)]
    outgoing = dispatch(ids, routed_rows).reshape(Z * X, 8, width)
    own = lax.all_to_all(outgoing, ep, split_axis=0, concat_axis=0, tiled=True).reshape(256, width)
    other = shifted(own, "c", C, 1)
    parts = expand(own, other, gate_weight[0], up_weight[0], shared)
    summed = [parts[0]] + [shifted(parts[s], "y", Y, Y - s) for s in (1, 2, 3)]
    mine = hidden_units(summed)
    units = [mine] + [shifted(mine, "y", Y, s) for s in (1, 2, 3)]
    own_out, other_out = reduce_units(units, down_weight[0], shared)
    other_out = shifted(other_out, "c", C, 1)
    result = added(own_out, other_out)
    returned = lax.all_to_all(
        result.reshape(Z * X, 8, width), ep, split_axis=0, concat_axis=0, tiled=True
    ).reshape(256, width)
    picked = collect(ids, returned)
    picked = [picked[0]] + [shifted(picked[s], "y", Y, s) for s in (1, 2, 3)]
    return finish(picked, route_weights)


def shards(
    queries,
    key_rows,
    value_rows,
    key_shift,
    out_weight,
    routed_rows,
    expert_ids,
    route_weights,
    gate_weight,
    up_weight,
    down_weight,
):
    mixed_rows = mixer(queries, key_rows, value_rows, key_shift, out_weight)
    routed_out = experts(routed_rows, expert_ids, route_weights, gate_weight, up_weight, down_weight)
    return (mixed_rows, routed_out)


def solution(mesh):
    mesh = Mesh(mesh.devices.reshape(Z, X, Y, C), ("z", "x", "y", "c"))
    ep, tp = ("z", "x"), ("y", "c")
    return jax.shard_map(
        shards,
        mesh=mesh,
        in_specs=(
            P(ep, tp),
            P(ep, tp),
            P(ep, tp),
            P(ep, tp),
            P(tp, None),
            P(ep, None),
            P(ep, None),
            P(ep + tp, None),
            P(ep, None, tp),
            P(ep, None, tp),
            P(ep, tp, None),
        ),
        out_specs=(P(ep + tp, None), P(ep + tp, None)),
        check_vma=False,
    )
```

```python
import jax
import jax.numpy as jnp
from jax import lax
from jax.experimental import pallas as pl
from jax.experimental.pallas import tpu as pltpu
from jax.sharding import Mesh, PartitionSpec as P


HEAD = 64
Z, X, Y, C = 8, 4, 4, 2
BF = jnp.bfloat16
F32 = jnp.float32

STEPS = (
    ((7, 6), (6, 5), (5, 4), (4, 3)),
    ((7, 5), (6, 4), (5, 3), (4, 2)),
    ((7, 4), (6, 3), (5, 2), (4, 1)),
    ((7, 3), (6, 2), (5, 1), (4, 0)),
    ((7, 2), (6, 1), (5, 0), (3, 2)),
    ((7, 1), (6, 0), (3, 1), (2, 1)),
    ((7, 0), (3, 0), (2, 0), (1, 0)),
)


def attend_kernel(*refs):
    arrived, (k1_ref, k2_ref, k3_ref, o_ref) = refs[:Z], refs[Z : Z + 4]
    attend_body(arrived, k1_ref, k2_ref, k3_ref, o_ref, *refs[Z + 4 :])


def attend_body(arrived, k1_ref, k2_ref, k3_ref, o_ref, kv_ref, qs_ref, tri_ref, carry_ref, acc_ref, steps_ref):
    here = lax.axis_index("x")
    plane = lax.axis_index("z")
    for i in range(Z):
        at = lax.rem(plane + (Z - i), Z)
        kv_ref[here, at] = arrived[i][HEAD:]
        for shift, piece in ((1, k1_ref), (2, k2_ref), (3, k3_ref)):
            kv_ref[lax.rem(here + (X - shift), X), at] = piece[i]
    row = lax.broadcasted_iota(jnp.int32, (256, 256), 0)
    col = lax.broadcasted_iota(jnp.int32, (256, 256), 1)
    tri_ref[...] = jnp.where(row > col, 1.0, 0.0).astype(BF)
    ones = jnp.where(lax.broadcasted_iota(jnp.int32, (64, 128), 0) == 0, 1.0, 0.0)
    for i in range(Z):
        q = jnp.concatenate([arrived[i][:HEAD].astype(F32), ones], axis=0)
        qs_ref[lax.rem(plane + (Z - i), Z)] = jnp.transpose(q).astype(BF)
    for i, step in enumerate(STEPS):
        for j, pair in enumerate(step):
            steps_ref[i, 2 * j] = pair[0]
            steps_ref[i, 2 * j + 1] = pair[1]

    def scores(b, t):
        keys = jnp.concatenate([kv_ref[i, t, 0:80, :] for i in range(4)], axis=1)
        return jnp.dot(qs_ref[b][:, 0:80], keys, preferred_element_type=F32)

    def tile(b, t, mask, carry):
        s = scores(b, t)
        sp = jnp.maximum(s, jnp.log(1.0 + jnp.exp(jnp.minimum(s, 80.0))))
        if mask is not None:
            sp = jnp.where(mask, sp, 0.0)
        rounded = sp.astype(BF)
        logit = s - sp
        weights = [None, None]
        for half in (1, 0):
            at = slice(half * 256, half * 256 + 256)
            behind = jnp.dot(rounded[:, at], tri_ref[...], preferred_element_type=F32)
            w = jnp.exp(logit[:, at] - behind - carry)
            if mask is not None:
                w = jnp.where(mask[:, at], w, 0.0)
            weights[half] = w.astype(BF)
            carry = carry + behind[:, 0:1] + sp[:, half * 256 : half * 256 + 1]
        values = jnp.concatenate([kv_ref[i, t, 80:144, :] for i in range(4)], axis=1)
        out = lax.dot_general(
            jnp.concatenate(weights, axis=1), values, (((1,), (1,)), ((), ())), preferred_element_type=F32
        )
        return out, carry

    def diagonal(i, unused):
        q_at = here * 128 + lax.broadcasted_iota(jnp.int32, (128, 512), 0)
        mask = lax.broadcasted_iota(jnp.int32, (128, 512), 1) < q_at
        done = [tile(i * 4 + j, i * 4 + j, mask, jnp.zeros((128, 1), F32)) for j in range(4)]
        for j in range(4):
            acc_ref[i * 4 + j] = done[j][0]
            carry_ref[i * 4 + j] = done[j][1]
        return unused

    lax.fori_loop(0, 2, diagonal, 0)

    def sweep(i, unused):
        blocks = [steps_ref[i, 2 * j] for j in range(4)]
        tiles = [steps_ref[i, 2 * j + 1] for j in range(4)]
        carries = [carry_ref[b] for b in blocks]
        before = [acc_ref[b] for b in blocks]
        done = [tile(blocks[j], tiles[j], None, carries[j]) for j in range(4)]
        for j in range(4):
            acc_ref[blocks[j]] = before[j] + done[j][0]
            carry_ref[blocks[j]] = done[j][1]
        return unused

    lax.fori_loop(0, len(STEPS), sweep, 0)
    for b in range(8):
        o_ref[b] = jnp.transpose(acc_ref[b]).astype(BF)


VMEM = pl.BlockSpec(memory_space=pltpu.VMEM)
ANY = pl.BlockSpec(memory_space=pl.ANY)


def attend(arrived, pieces):
    return pl.pallas_call(
        attend_kernel,
        out_shape=jax.ShapeDtypeStruct((8, HEAD, 128), BF),
        in_specs=[VMEM] * (Z + 3),
        out_specs=VMEM,
        scratch_shapes=[
            pltpu.VMEM((4, 8, 144, 128), BF),
            pltpu.VMEM((8, 128, 128), BF),
            pltpu.VMEM((256, 256), BF),
            pltpu.VMEM((8, 128, 1), F32),
            pltpu.VMEM((8, 128, HEAD), F32),
            pltpu.SMEM((len(STEPS), 8), jnp.int32),
        ],
        compiler_params=pltpu.CompilerParams(vmem_limit_bytes=32 * 1024 * 1024),
        cost_estimate=pl.CostEstimate(flops=4_000_000_000, transcendentals=7_000_000, bytes_accessed=2_000_000),
    )(*arrived, *pieces)


def pack_kernel(q_ref, k_ref, v_ref, shift_ref, *refs):
    outs, (q_all, k_all, v_all, shift_all) = refs[:Z], refs[Z:]
    plane = lax.axis_index("z")
    q_all[...] = jnp.transpose(q_ref[...].astype(F32) * HEAD**-0.5)
    k_all[...] = jnp.transpose(k_ref[...].astype(F32))
    v_all[...] = jnp.transpose(v_ref[...].astype(F32))
    shift_all[...] = shift_ref[...].astype(F32)
    first = lax.broadcasted_iota(jnp.int32, (16, 128), 0) == 0
    for s, out in enumerate(outs):
        head = lax.rem(plane + s, Z)
        rows = pl.ds(pl.multiple_of(head * HEAD, HEAD), HEAD)
        out[0:64] = q_all[rows, :].astype(BF)
        out[64:128] = k_all[rows, :].astype(BF)
        shift = jnp.broadcast_to(shift_all[pl.ds(head, 1), :], (16, 128))
        out[128:144] = jnp.where(first, shift, 0.0).astype(BF)
        out[144:208] = v_all[rows, :].astype(BF)


def stack_kernel(*refs):
    for i in range(Z):
        refs[Z][i] = refs[i][HEAD:]


def stacked(arrived):
    return pl.pallas_call(
        stack_kernel,
        out_shape=jax.ShapeDtypeStruct((Z, 144, 128), BF),
        in_specs=[VMEM] * Z,
        out_specs=VMEM,
    )(*arrived)


def pack(queries, key_rows, value_rows, shift):
    rows, width = queries.shape
    return pl.pallas_call(
        pack_kernel,
        out_shape=[jax.ShapeDtypeStruct((208, 128), BF)] * Z,
        in_specs=[VMEM] * 4,
        out_specs=[VMEM] * Z,
        scratch_shapes=[pltpu.VMEM((width, rows), F32)] * 3 + [pltpu.VMEM((8, rows), F32)],
    )(queries, key_rows, value_rows, shift)


def shifted(value, axis, size, by):
    return lax.ppermute(value, axis, [(i, (i + by) % size) for i in range(size)])


def mixer(queries, key_rows, value_rows, key_shift, out_weight):
    heads = key_shift.shape[1]
    rows = queries.shape[0]
    packed = pack(queries, key_rows, value_rows, key_shift.T)
    arrived = [packed[0]] + [shifted(packed[by], "z", Z, by) for by in range(1, Z)]
    keys = stacked(arrived)
    pieces = [shifted(keys, "x", X, by) for by in (1, 2, 3)]
    out = attend(arrived, pieces)
    attended = lax.all_to_all(out, "z", split_axis=0, concat_axis=0, tiled=True)
    attended = attended.reshape(heads * HEAD, rows)
    partial = lax.dot_general(
        attended, out_weight, (((0,), (0,)), ((), ())), preferred_element_type=F32
    ).astype(BF)
    return summed_over_tp(partial)


def summed_over_tp(partial):
    y, core = lax.axis_index("y"), lax.axis_index("c")
    rows, width = partial.shape
    per = rows // (Y * C)
    parts = partial.reshape(Y, C, per, width)
    mine = lax.dynamic_index_in_dim(parts, core, 1, keepdims=False)
    other = lax.dynamic_index_in_dim(parts, 1 - core, 1, keepdims=False)
    both = (mine.astype(F32) + shifted(other, "c", C, 1).astype(F32)).astype(BF)
    total = lax.dynamic_index_in_dim(both, y, 0, keepdims=False).astype(F32)
    for by in (1, 2, 3):
        piece = lax.dynamic_index_in_dim(both, lax.rem(y + by, Y), 0, keepdims=False)
        total = total + shifted(piece, "y", Y, by).astype(F32)
    return total.astype(BF)


def selection(ids_ref, core):
    row = lax.broadcasted_iota(jnp.int32, (256, 128), 0)
    token = lax.broadcasted_iota(jnp.int32, (256, 128), 1)
    expert = lax.div(row, 8)
    named = [ids_ref[k : k + 1, :] == expert for k in range(2)]
    either = jnp.where(named[0] | named[1], 1.0, 0.0)
    before = lax.broadcasted_iota(jnp.int32, (128, 128), 0)
    after = lax.broadcasted_iota(jnp.int32, (128, 128), 1)
    earlier = jnp.where((before < after) & (lax.div(before, 16) == lax.div(after, 16)), 1.0, 0.0)
    slot = jnp.dot(either.astype(BF), earlier.astype(BF), preferred_element_type=F32)
    here = (lax.div(token, 16) == 2 * lax.div(lax.rem(row, 8), 2) + core) & (
        slot == lax.rem(row, 2).astype(F32)
    )
    return [jnp.where(n & here, 1.0, 0.0) for n in named]


def dispatch_kernel(ids_ref, rows_ref, out_ref, part_ref, sem):
    width = out_ref.shape[1]
    start = pl.multiple_of(lax.axis_index("y") * width, width)
    copy = pltpu.make_async_copy(rows_ref.at[:, pl.ds(start, width)], part_ref, sem)
    copy.start()
    first, second = selection(ids_ref, lax.axis_index("c"))
    pick = (first + second).astype(BF)
    copy.wait()
    out_ref[...] = jnp.dot(pick, part_ref[...], preferred_element_type=F32).astype(BF)


def dispatch(ids, rows):
    width = rows.shape[1] // Y
    return pl.pallas_call(
        dispatch_kernel,
        out_shape=jax.ShapeDtypeStruct((256, width), BF),
        in_specs=[VMEM, ANY],
        out_specs=VMEM,
        scratch_shapes=[pltpu.VMEM((128, width), BF), pltpu.SemaphoreType.DMA],
    )(ids, rows)


def collect_kernel(ids_ref, rows_ref, o0_ref, o1_ref, o2_ref, o3_ref, all_ref):
    y, core = lax.axis_index("y"), lax.axis_index("c")
    for k, pick in enumerate(selection(ids_ref, core)):
        chosen = jnp.transpose(pick).astype(BF)
        all_ref[k] = jnp.dot(chosen, rows_ref[...], preferred_element_type=F32).astype(BF)
        for s, out in enumerate((o0_ref, o1_ref, o2_ref, o3_ref)):
            at = pl.multiple_of((2 * lax.rem(y + s, Y) + core) * 16, 16)
            out[k] = all_ref[k, pl.ds(at, 16), :]


def collect(ids, rows):
    width = rows.shape[1]
    return pl.pallas_call(
        collect_kernel,
        out_shape=[jax.ShapeDtypeStruct((2, 16, width), BF)] * Y,
        in_specs=[VMEM, VMEM],
        out_specs=[VMEM] * Y,
        scratch_shapes=[pltpu.VMEM((2, 128, width), BF)],
    )(ids, rows)


def spread_kernel(weights_ref, out_ref):
    w = weights_ref[...]
    for k in range(2):
        out_ref[k] = jnp.broadcast_to(w[:, k : k + 1], (16, 128))


def spread_weights(weights):
    return pl.pallas_call(
        spread_kernel,
        out_shape=jax.ShapeDtypeStruct((2, 16, 128), F32),
        in_specs=[VMEM],
        out_specs=VMEM,
    )(weights)


def finish_kernel(p0_ref, p1_ref, p2_ref, p3_ref, weights_ref, out_ref):
    width = p0_ref.shape[2]
    w = [jnp.concatenate([weights_ref[k]] * (width // 128), axis=1) for k in range(2)]
    for s, p in enumerate((p0_ref, p1_ref, p2_ref, p3_ref)):
        at = pl.multiple_of(lax.rem(lax.axis_index("y") + (Y - s), Y) * width, width)
        total = p[0].astype(F32) * w[0] + p[1].astype(F32) * w[1]
        out_ref[:, pl.ds(at, width)] = total.astype(BF)


def finish(picked, weights):
    return pl.pallas_call(
        finish_kernel,
        out_shape=jax.ShapeDtypeStruct((16, Y * picked[0].shape[2]), BF),
        in_specs=[VMEM] * 5,
        out_specs=VMEM,
    )(*picked, weights)


def share_kernel(gate_ref, up_ref, down_ref, o0_ref, o1_ref, o2_ref, o3_ref, sem):
    width = gate_ref.shape[0] // Y
    copies = []
    for s, out in ((1, o1_ref), (2, o2_ref), (3, o3_ref), (0, o0_ref)):
        start = pl.multiple_of(lax.rem(lax.axis_index("y") + s, Y) * width, width)
        copies.append((gate_ref.at[pl.ds(start, width), :], out.at[pl.ds(0, width), :]))
        copies.append((up_ref.at[pl.ds(start, width), :], out.at[pl.ds(width, width), :]))
        for j in range(width // 128):
            copies.append(
                (
                    down_ref.at[:, pl.ds(pl.multiple_of(start + j * 128, 128), 128)],
                    out.at[pl.ds(2 * width + j * 128, 128), :],
                )
            )
    made = [pltpu.make_async_copy(a, b, sem.at[n]) for n, (a, b) in enumerate(copies)]
    for m in made:
        m.start()
    for m in made:
        m.wait()


def share(gate, up, down):
    width = gate.shape[0] // Y
    out = jax.ShapeDtypeStruct((3 * width, 128), BF)
    return pl.pallas_call(
        share_kernel,
        out_shape=[out] * Y,
        in_specs=[ANY, ANY, ANY],
        out_specs=[VMEM] * Y,
        scratch_shapes=[pltpu.SemaphoreType.DMA((Y * (2 + width // 128),))],
    )(gate, up, down)


def expand_kernel(*refs):
    rows_ref, ours, theirs, outs = refs[0], refs[1 : 1 + Y], refs[1 + Y : 1 + 2 * Y], refs[1 + 2 * Y :]
    width = rows_ref.shape[1]
    for s in (1, 2, 3, 0):
        parts = []
        for w_ref in (ours[s], theirs[s]):
            w = jnp.concatenate([w_ref[0:width], w_ref[width : 2 * width]], axis=1)
            parts.append(jnp.dot(rows_ref[...], w, preferred_element_type=F32))
        outs[s][...] = jnp.concatenate(parts, axis=1).astype(outs[s].dtype)


def expand(rows, ours, theirs):
    sent = jax.ShapeDtypeStruct((rows.shape[0], 512), BF)
    return pl.pallas_call(
        expand_kernel,
        out_shape=[jax.ShapeDtypeStruct((rows.shape[0], 512), F32), sent, sent, sent],
        in_specs=[VMEM] * (1 + 2 * Y),
        out_specs=[VMEM] * Y,
        compiler_params=pltpu.CompilerParams(vmem_limit_bytes=32 * 1024 * 1024),
    )(rows, *ours, *theirs)


def hidden_kernel(p0_ref, p1_ref, p2_ref, p3_ref, o_ref):
    for n in range(C):
        both = p0_ref[:, n * 256 : n * 256 + 256]
        for p in (p1_ref, p2_ref, p3_ref):
            both = both + p[:, n * 256 : n * 256 + 256].astype(F32)
        gate, up = both[:, 0:128], both[:, 128:256]
        o_ref[:, n * 128 : n * 128 + 128] = (gate / (1.0 + jnp.exp(-gate)) * up).astype(BF)


def hidden_units(parts):
    return pl.pallas_call(
        hidden_kernel,
        out_shape=jax.ShapeDtypeStruct((parts[0].shape[0], 256), BF),
        in_specs=[VMEM] * 4,
        out_specs=VMEM,
    )(*parts)


def reduce_kernel(*refs):
    units, ours, theirs, o_ref = refs[:Y], refs[Y : 2 * Y], refs[2 * Y : 3 * Y], refs[3 * Y]
    width = o_ref.shape[1]
    columns = []
    for s in range(Y):
        for w_ref in (ours[s], theirs[s]):
            blocks = [w_ref[2 * width + j * 128 : 2 * width + j * 128 + 128] for j in range(width // 128)]
            columns.append(jnp.concatenate(blocks, axis=1))
    w = jnp.concatenate(columns, axis=0)
    h = jnp.concatenate([u[...] for u in units], axis=1)
    o_ref[...] = jnp.dot(h, w, preferred_element_type=F32).astype(BF)


def reduce_units(units, ours, theirs):
    rows = units[0].shape[0]
    width = ours[0].shape[0] // 3
    return pl.pallas_call(
        reduce_kernel,
        out_shape=jax.ShapeDtypeStruct((rows, width), BF),
        in_specs=[VMEM] * (3 * Y),
        out_specs=VMEM,
        compiler_params=pltpu.CompilerParams(vmem_limit_bytes=32 * 1024 * 1024),
    )(*units, *ours, *theirs)


def experts(routed_rows, expert_ids, route_weights, gate_weight, up_weight, down_weight):
    ep = ("z", "x")
    ids = expert_ids.T
    width = routed_rows.shape[1] // Y
    kept = share(gate_weight[0], up_weight[0], down_weight[0])
    ours = [kept[0]] + [shifted(kept[s], "y", Y, s) for s in (1, 2, 3)]
    theirs = [shifted(w, "c", C, 1) for w in ours]
    outgoing = dispatch(ids, routed_rows).reshape(Z * X, 8, width)
    own = lax.all_to_all(outgoing, ep, split_axis=0, concat_axis=0, tiled=True).reshape(256, width)
    wide = spread_weights(route_weights)
    parts = expand(own, ours, theirs)
    summed = [parts[0]] + [shifted(parts[s], "y", Y, Y - s) for s in (1, 2, 3)]
    mine = hidden_units(summed)
    units = [mine] + [shifted(mine, "y", Y, s) for s in (1, 2, 3)]
    result = reduce_units(units, ours, theirs)
    returned = lax.all_to_all(
        result.reshape(Z * X, 8, width), ep, split_axis=0, concat_axis=0, tiled=True
    ).reshape(256, width)
    picked = collect(ids, returned)
    picked = [picked[0]] + [shifted(picked[s], "y", Y, s) for s in (1, 2, 3)]
    return finish(picked, wide)


def shards(
    queries,
    key_rows,
    value_rows,
    key_shift,
    out_weight,
    routed_rows,
    expert_ids,
    route_weights,
    gate_weight,
    up_weight,
    down_weight,
):
    mixed_rows = mixer(queries, key_rows, value_rows, key_shift, out_weight)
    routed_out = experts(routed_rows, expert_ids, route_weights, gate_weight, up_weight, down_weight)
    return (mixed_rows, routed_out)


def solution(mesh):
    mesh = Mesh(mesh.devices.reshape(Z, X, Y, C), ("z", "x", "y", "c"))
    ep, tp = ("z", "x"), ("y", "c")
    return jax.shard_map(
        shards,
        mesh=mesh,
        in_specs=(
            P(ep, tp),
            P(ep, tp),
            P(ep, tp),
            P(ep, tp),
            P(tp, None),
            P(ep, None),
            P(ep, None),
            P(ep + tp, None),
            P(ep, None, tp),
            P(ep, None, tp),
            P(ep, tp, None),
        ),
        out_specs=(P(ep + tp, None), P(ep + tp, None)),
        check_vma=False,
    )
```

```python
import jax
import jax.numpy as jnp
from jax import lax
from jax.experimental import pallas as pl
from jax.experimental.pallas import tpu as pltpu
from jax.sharding import Mesh, PartitionSpec as P


HEAD = 64
Z, X, Y, C = 8, 4, 4, 2
BF = jnp.bfloat16
MIB = 1024 * 1024
F32 = jnp.float32

STEPS = (
    ((7, 6), (6, 5), (5, 4), (4, 3)),
    ((7, 5), (6, 4), (5, 3), (4, 2)),
    ((7, 4), (6, 3), (5, 2), (4, 1)),
    ((7, 3), (6, 2), (5, 1), (4, 0)),
    ((7, 2), (6, 1), (5, 0), (3, 2)),
    ((7, 1), (6, 0), (3, 1), (2, 1)),
    ((7, 0), (3, 0), (2, 0), (1, 0)),
)


def attend_kernel(*refs):
    arrived, (k1_ref, k2_ref, k3_ref, o_ref) = refs[:Z], refs[Z : Z + 4]
    attend_body(arrived, k1_ref, k2_ref, k3_ref, o_ref, *refs[Z + 4 :])


def attend_body(arrived, k1_ref, k2_ref, k3_ref, o_ref, kv_ref, qs_ref, tri_ref, carry_ref, acc_ref, steps_ref):
    here = lax.axis_index("x")
    plane = lax.axis_index("z")
    for i in range(Z):
        at = lax.rem(plane + (Z - i), Z)
        kv_ref[here, at] = arrived[i][HEAD:]
        for shift, piece in ((1, k1_ref), (2, k2_ref), (3, k3_ref)):
            kv_ref[lax.rem(here + (X - shift), X), at] = piece[i]
    row = lax.broadcasted_iota(jnp.int32, (256, 256), 0)
    col = lax.broadcasted_iota(jnp.int32, (256, 256), 1)
    tri_ref[...] = jnp.where(row > col, 1.0, 0.0).astype(BF)
    ones = jnp.where(lax.broadcasted_iota(jnp.int32, (64, 128), 0) == 0, 1.0, 0.0)
    for i in range(Z):
        q = jnp.concatenate([arrived[i][:HEAD].astype(F32), ones], axis=0)
        qs_ref[lax.rem(plane + (Z - i), Z)] = jnp.transpose(q).astype(BF)
    for i, step in enumerate(STEPS):
        for j, pair in enumerate(step):
            steps_ref[i, 2 * j] = pair[0]
            steps_ref[i, 2 * j + 1] = pair[1]

    def scores(b, t):
        keys = jnp.concatenate([kv_ref[i, t, 0:80, :] for i in range(4)], axis=1)
        return jnp.dot(qs_ref[b][:, 0:80], keys, preferred_element_type=F32)

    def tile(b, t, mask, carry):
        s = scores(b, t)
        sp = jnp.maximum(s, jnp.log(1.0 + jnp.exp(jnp.minimum(s, 80.0))))
        if mask is not None:
            sp = jnp.where(mask, sp, 0.0)
        rounded = sp.astype(BF)
        logit = s - sp
        weights = [None, None]
        for half in (1, 0):
            at = slice(half * 256, half * 256 + 256)
            behind = jnp.dot(rounded[:, at], tri_ref[...], preferred_element_type=F32)
            w = jnp.exp(logit[:, at] - behind - carry)
            if mask is not None:
                w = jnp.where(mask[:, at], w, 0.0)
            weights[half] = w.astype(BF)
            carry = carry + behind[:, 0:1] + sp[:, half * 256 : half * 256 + 1]
        values = jnp.concatenate([kv_ref[i, t, 80:144, :] for i in range(4)], axis=1)
        out = lax.dot_general(
            jnp.concatenate(weights, axis=1), values, (((1,), (1,)), ((), ())), preferred_element_type=F32
        )
        return out, carry

    def diagonal(i, unused):
        q_at = here * 128 + lax.broadcasted_iota(jnp.int32, (128, 512), 0)
        mask = lax.broadcasted_iota(jnp.int32, (128, 512), 1) < q_at
        done = [tile(i * 4 + j, i * 4 + j, mask, jnp.zeros((128, 1), F32)) for j in range(4)]
        for j in range(4):
            acc_ref[i * 4 + j] = done[j][0]
            carry_ref[i * 4 + j] = done[j][1]
        return unused

    lax.fori_loop(0, 2, diagonal, 0)

    def sweep(i, unused):
        blocks = [steps_ref[i, 2 * j] for j in range(4)]
        tiles = [steps_ref[i, 2 * j + 1] for j in range(4)]
        carries = [carry_ref[b] for b in blocks]
        before = [acc_ref[b] for b in blocks]
        done = [tile(blocks[j], tiles[j], None, carries[j]) for j in range(4)]
        for j in range(4):
            acc_ref[blocks[j]] = before[j] + done[j][0]
            carry_ref[blocks[j]] = done[j][1]
        return unused

    lax.fori_loop(0, len(STEPS), sweep, 0)
    for b in range(8):
        o_ref[b] = jnp.transpose(acc_ref[b]).astype(BF)


VMEM = pl.BlockSpec(memory_space=pltpu.VMEM)
ANY = pl.BlockSpec(memory_space=pl.ANY)


def attend(arrived, pieces):
    return pl.pallas_call(
        attend_kernel,
        out_shape=jax.ShapeDtypeStruct((8, HEAD, 128), BF),
        in_specs=[VMEM] * (Z + 3),
        out_specs=VMEM,
        scratch_shapes=[
            pltpu.VMEM((4, 8, 144, 128), BF),
            pltpu.VMEM((8, 128, 128), BF),
            pltpu.VMEM((256, 256), BF),
            pltpu.VMEM((8, 128, 1), F32),
            pltpu.VMEM((8, 128, HEAD), F32),
            pltpu.SMEM((len(STEPS), 8), jnp.int32),
        ],
        compiler_params=pltpu.CompilerParams(vmem_limit_bytes=14 * MIB),
        cost_estimate=pl.CostEstimate(flops=4_000_000_000, transcendentals=7_000_000, bytes_accessed=2_000_000),
    )(*arrived, *pieces)


def pack_kernel(q_ref, k_ref, v_ref, shift_ref, *refs):
    outs, (q_all, k_all, v_all, shift_all) = refs[:Z], refs[Z:]
    plane = lax.axis_index("z")
    q_all[...] = jnp.transpose(q_ref[...].astype(F32) * HEAD**-0.5)
    k_all[...] = jnp.transpose(k_ref[...].astype(F32))
    v_all[...] = jnp.transpose(v_ref[...].astype(F32))
    shift_all[...] = shift_ref[...].astype(F32)
    first = lax.broadcasted_iota(jnp.int32, (16, 128), 0) == 0
    for s, out in enumerate(outs):
        head = lax.rem(plane + s, Z)
        rows = pl.ds(pl.multiple_of(head * HEAD, HEAD), HEAD)
        out[0:64] = q_all[rows, :].astype(BF)
        out[64:128] = k_all[rows, :].astype(BF)
        shift = jnp.broadcast_to(shift_all[pl.ds(head, 1), :], (16, 128))
        out[128:144] = jnp.where(first, shift, 0.0).astype(BF)
        out[144:208] = v_all[rows, :].astype(BF)


def stack_kernel(*refs):
    for i in range(Z):
        refs[Z][i] = refs[i][HEAD:]


def stacked(arrived):
    return pl.pallas_call(
        stack_kernel,
        out_shape=jax.ShapeDtypeStruct((Z, 144, 128), BF),
        in_specs=[VMEM] * Z,
        out_specs=VMEM,
    )(*arrived)


def pack(queries, key_rows, value_rows, shift):
    rows, width = queries.shape
    return pl.pallas_call(
        pack_kernel,
        out_shape=[jax.ShapeDtypeStruct((208, 128), BF)] * Z,
        in_specs=[VMEM] * 4,
        out_specs=[VMEM] * Z,
        scratch_shapes=[pltpu.VMEM((width, rows), F32)] * 3 + [pltpu.VMEM((8, rows), F32)],
    )(queries, key_rows, value_rows, shift)


def shifted(value, axis, size, by):
    return lax.ppermute(value, axis, [(i, (i + by) % size) for i in range(size)])


def mixer(queries, key_rows, value_rows, key_shift, out_weight):
    heads = key_shift.shape[1]
    rows = queries.shape[0]
    packed = pack(queries, key_rows, value_rows, key_shift.T)
    arrived = [packed[0]] + [shifted(packed[by], "z", Z, by) for by in range(1, Z)]
    keys = stacked(arrived)
    pieces = [shifted(keys, "x", X, by) for by in (1, 2, 3)]
    out = attend(arrived, pieces)
    attended = lax.all_to_all(out, "z", split_axis=0, concat_axis=0, tiled=True)
    attended = attended.reshape(heads * HEAD, rows)
    partial = lax.dot_general(
        attended, out_weight, (((0,), (0,)), ((), ())), preferred_element_type=F32
    ).astype(BF)
    return summed_over_tp(partial)


def summed_over_tp(partial):
    y, core = lax.axis_index("y"), lax.axis_index("c")
    rows, width = partial.shape
    per = rows // (Y * C)
    parts = partial.reshape(Y, C, per, width)
    mine = lax.dynamic_index_in_dim(parts, core, 1, keepdims=False)
    other = lax.dynamic_index_in_dim(parts, 1 - core, 1, keepdims=False)
    both = (mine.astype(F32) + shifted(other, "c", C, 1).astype(F32)).astype(BF)
    total = lax.dynamic_index_in_dim(both, y, 0, keepdims=False).astype(F32)
    for by in (1, 2, 3):
        piece = lax.dynamic_index_in_dim(both, lax.rem(y + by, Y), 0, keepdims=False)
        total = total + shifted(piece, "y", Y, by).astype(F32)
    return total.astype(BF)


def selection(ids_ref, core):
    row = lax.broadcasted_iota(jnp.int32, (256, 128), 0)
    token = lax.broadcasted_iota(jnp.int32, (256, 128), 1)
    expert = lax.div(row, 8)
    named = [ids_ref[k : k + 1, :] == expert for k in range(2)]
    either = jnp.where(named[0] | named[1], 1.0, 0.0)
    before = lax.broadcasted_iota(jnp.int32, (128, 128), 0)
    after = lax.broadcasted_iota(jnp.int32, (128, 128), 1)
    earlier = jnp.where((before < after) & (lax.div(before, 16) == lax.div(after, 16)), 1.0, 0.0)
    slot = jnp.dot(either.astype(BF), earlier.astype(BF), preferred_element_type=F32)
    here = (lax.div(token, 16) == 2 * lax.div(lax.rem(row, 8), 2) + core) & (
        slot == lax.rem(row, 2).astype(F32)
    )
    return [jnp.where(n & here, 1.0, 0.0) for n in named]


def dispatch_kernel(ids_ref, rows_ref, out_ref, part_ref, sem):
    width = out_ref.shape[1]
    start = pl.multiple_of(lax.axis_index("y") * width, width)
    copy = pltpu.make_async_copy(rows_ref.at[:, pl.ds(start, width)], part_ref, sem)
    copy.start()
    first, second = selection(ids_ref, lax.axis_index("c"))
    pick = (first + second).astype(BF)
    copy.wait()
    out_ref[...] = jnp.dot(pick, part_ref[...], preferred_element_type=F32).astype(BF)


def dispatch(ids, rows):
    width = rows.shape[1] // Y
    return pl.pallas_call(
        dispatch_kernel,
        out_shape=jax.ShapeDtypeStruct((256, width), BF),
        in_specs=[VMEM, ANY],
        out_specs=VMEM,
        scratch_shapes=[pltpu.VMEM((128, width), BF), pltpu.SemaphoreType.DMA],
    )(ids, rows)


def collect_kernel(ids_ref, rows_ref, o0_ref, o1_ref, o2_ref, o3_ref, all_ref):
    y, core = lax.axis_index("y"), lax.axis_index("c")
    for k, pick in enumerate(selection(ids_ref, core)):
        chosen = jnp.transpose(pick).astype(BF)
        all_ref[k] = jnp.dot(chosen, rows_ref[...], preferred_element_type=F32).astype(BF)
        for s, out in enumerate((o0_ref, o1_ref, o2_ref, o3_ref)):
            at = pl.multiple_of((2 * lax.rem(y + s, Y) + core) * 16, 16)
            out[k] = all_ref[k, pl.ds(at, 16), :]


def collect(ids, rows):
    width = rows.shape[1]
    return pl.pallas_call(
        collect_kernel,
        out_shape=[jax.ShapeDtypeStruct((2, 16, width), BF)] * Y,
        in_specs=[VMEM, VMEM],
        out_specs=[VMEM] * Y,
        scratch_shapes=[pltpu.VMEM((2, 128, width), BF)],
        compiler_params=pltpu.CompilerParams(vmem_limit_bytes=5 * MIB),
    )(ids, rows)


def spread_kernel(weights_ref, out_ref):
    w = weights_ref[...]
    for k in range(2):
        out_ref[k] = jnp.broadcast_to(w[:, k : k + 1], (16, 128))


def spread_weights(weights):
    return pl.pallas_call(
        spread_kernel,
        out_shape=jax.ShapeDtypeStruct((2, 16, 128), F32),
        in_specs=[VMEM],
        out_specs=VMEM,
    )(weights)


def finish_kernel(p0_ref, p1_ref, p2_ref, p3_ref, weights_ref, out_ref):
    width = p0_ref.shape[2]
    w = [jnp.concatenate([weights_ref[k]] * (width // 128), axis=1) for k in range(2)]
    for s, p in enumerate((p0_ref, p1_ref, p2_ref, p3_ref)):
        at = pl.multiple_of(lax.rem(lax.axis_index("y") + (Y - s), Y) * width, width)
        total = p[0].astype(F32) * w[0] + p[1].astype(F32) * w[1]
        out_ref[:, pl.ds(at, width)] = total.astype(BF)


def finish(picked, weights):
    return pl.pallas_call(
        finish_kernel,
        out_shape=jax.ShapeDtypeStruct((16, Y * picked[0].shape[2]), BF),
        in_specs=[VMEM] * 5,
        out_specs=VMEM,
        compiler_params=pltpu.CompilerParams(vmem_limit_bytes=4 * MIB),
    )(*picked, weights)


def share_kernel(gate_ref, up_ref, down_ref, o0_ref, o1_ref, o2_ref, o3_ref, sem):
    width = gate_ref.shape[0] // Y
    copies = []
    for s, out in ((1, o1_ref), (2, o2_ref), (3, o3_ref), (0, o0_ref)):
        start = pl.multiple_of(lax.rem(lax.axis_index("y") + s, Y) * width, width)
        copies.append((gate_ref.at[pl.ds(start, width), :], out.at[pl.ds(0, width), :]))
        copies.append((up_ref.at[pl.ds(start, width), :], out.at[pl.ds(width, width), :]))
        for j in range(width // 128):
            copies.append(
                (
                    down_ref.at[:, pl.ds(pl.multiple_of(start + j * 128, 128), 128)],
                    out.at[pl.ds(2 * width + j * 128, 128), :],
                )
            )
    made = [pltpu.make_async_copy(a, b, sem.at[n]) for n, (a, b) in enumerate(copies)]
    for m in made:
        m.start()
    for m in made:
        m.wait()


def share(gate, up, down):
    width = gate.shape[0] // Y
    out = jax.ShapeDtypeStruct((3 * width, 128), BF)
    return pl.pallas_call(
        share_kernel,
        out_shape=[out] * Y,
        in_specs=[ANY, ANY, ANY],
        out_specs=[VMEM] * Y,
        scratch_shapes=[pltpu.SemaphoreType.DMA((Y * (2 + width // 128),))],
    )(gate, up, down)


def expand_kernel(*refs):
    rows_ref, ours, theirs, outs = refs[0], refs[1 : 1 + Y], refs[1 + Y : 1 + 2 * Y], refs[1 + 2 * Y :]
    width = rows_ref.shape[1]
    for s in (1, 2, 3, 0):
        parts = []
        for w_ref in (ours[s], theirs[s]):
            w = jnp.concatenate([w_ref[0:width], w_ref[width : 2 * width]], axis=1)
            parts.append(jnp.dot(rows_ref[...], w, preferred_element_type=F32))
        outs[s][...] = jnp.concatenate(parts, axis=1).astype(outs[s].dtype)


def expand(rows, ours, theirs):
    sent = jax.ShapeDtypeStruct((rows.shape[0], 512), BF)
    return pl.pallas_call(
        expand_kernel,
        out_shape=[jax.ShapeDtypeStruct((rows.shape[0], 512), F32), sent, sent, sent],
        in_specs=[VMEM] * (1 + 2 * Y),
        out_specs=[VMEM] * Y,
        compiler_params=pltpu.CompilerParams(vmem_limit_bytes=16 * MIB),
    )(rows, *ours, *theirs)


def hidden_kernel(p0_ref, p1_ref, p2_ref, p3_ref, o_ref):
    for n in range(C):
        both = p0_ref[:, n * 256 : n * 256 + 256]
        for p in (p1_ref, p2_ref, p3_ref):
            both = both + p[:, n * 256 : n * 256 + 256].astype(F32)
        gate, up = both[:, 0:128], both[:, 128:256]
        o_ref[:, n * 128 : n * 128 + 128] = (gate / (1.0 + jnp.exp(-gate)) * up).astype(BF)


def hidden_units(parts):
    return pl.pallas_call(
        hidden_kernel,
        out_shape=jax.ShapeDtypeStruct((parts[0].shape[0], 256), BF),
        in_specs=[VMEM] * 4,
        out_specs=VMEM,
        compiler_params=pltpu.CompilerParams(vmem_limit_bytes=5 * MIB),
    )(*parts)


def reduce_kernel(*refs):
    units, ours, theirs, o_ref = refs[:Y], refs[Y : 2 * Y], refs[2 * Y : 3 * Y], refs[3 * Y]
    width = o_ref.shape[1]
    columns = []
    for s in range(Y):
        for w_ref in (ours[s], theirs[s]):
            blocks = [w_ref[2 * width + j * 128 : 2 * width + j * 128 + 128] for j in range(width // 128)]
            columns.append(jnp.concatenate(blocks, axis=1))
    w = jnp.concatenate(columns, axis=0)
    h = jnp.concatenate([u[...] for u in units], axis=1)
    o_ref[...] = jnp.dot(h, w, preferred_element_type=F32).astype(BF)


def reduce_units(units, ours, theirs):
    rows = units[0].shape[0]
    width = ours[0].shape[0] // 3
    return pl.pallas_call(
        reduce_kernel,
        out_shape=jax.ShapeDtypeStruct((rows, width), BF),
        in_specs=[VMEM] * (3 * Y),
        out_specs=VMEM,
        compiler_params=pltpu.CompilerParams(vmem_limit_bytes=16 * MIB),
    )(*units, *ours, *theirs)


def experts(routed_rows, expert_ids, route_weights, gate_weight, up_weight, down_weight):
    ep = ("z", "x")
    ids = expert_ids.T
    width = routed_rows.shape[1] // Y
    kept = share(gate_weight[0], up_weight[0], down_weight[0])
    ours = [kept[0]] + [shifted(kept[s], "y", Y, s) for s in (1, 2, 3)]
    theirs = [shifted(w, "c", C, 1) for w in ours]
    outgoing = dispatch(ids, routed_rows).reshape(Z * X, 8, width)
    own = lax.all_to_all(outgoing, ep, split_axis=0, concat_axis=0, tiled=True).reshape(256, width)
    wide = spread_weights(route_weights)
    parts = expand(own, ours, theirs)
    summed = [parts[0]] + [shifted(parts[s], "y", Y, Y - s) for s in (1, 2, 3)]
    mine = hidden_units(summed)
    units = [mine] + [shifted(mine, "y", Y, s) for s in (1, 2, 3)]
    result = reduce_units(units, ours, theirs)
    returned = lax.all_to_all(
        result.reshape(Z * X, 8, width), ep, split_axis=0, concat_axis=0, tiled=True
    ).reshape(256, width)
    picked = collect(ids, returned)
    picked = [picked[0]] + [shifted(picked[s], "y", Y, s) for s in (1, 2, 3)]
    return finish(picked, wide)


def shards(
    queries,
    key_rows,
    value_rows,
    key_shift,
    out_weight,
    routed_rows,
    expert_ids,
    route_weights,
    gate_weight,
    up_weight,
    down_weight,
):
    mixed_rows = mixer(queries, key_rows, value_rows, key_shift, out_weight)
    routed_out = experts(routed_rows, expert_ids, route_weights, gate_weight, up_weight, down_weight)
    return (mixed_rows, routed_out)


def solution(mesh):
    mesh = Mesh(mesh.devices.reshape(Z, X, Y, C), ("z", "x", "y", "c"))
    ep, tp = ("z", "x"), ("y", "c")
    return jax.shard_map(
        shards,
        mesh=mesh,
        in_specs=(
            P(ep, tp),
            P(ep, tp),
            P(ep, tp),
            P(ep, tp),
            P(tp, None),
            P(ep, None),
            P(ep, None),
            P(ep + tp, None),
            P(ep, None, tp),
            P(ep, None, tp),
            P(ep, tp, None),
        ),
        out_specs=(P(ep + tp, None), P(ep + tp, None)),
        check_vma=False,
    )
```

```python
import jax
import jax.numpy as jnp
from jax import lax
from jax.experimental import pallas as pl
from jax.experimental.pallas import tpu as pltpu
from jax.sharding import Mesh, PartitionSpec as P


HEAD = 64
Z, X, Y, C = 8, 4, 4, 2
BF = jnp.bfloat16
MIB = 1024 * 1024
F32 = jnp.float32

STEPS = (
    ((7, 6), (6, 5), (5, 4), (4, 3)),
    ((7, 5), (6, 4), (5, 3), (4, 2)),
    ((7, 4), (6, 3), (5, 2), (4, 1)),
    ((7, 3), (6, 2), (5, 1), (4, 0)),
    ((7, 2), (6, 1), (5, 0), (3, 2)),
    ((7, 1), (6, 0), (3, 1), (2, 1)),
    ((7, 0), (3, 0), (2, 0), (1, 0)),
)


def attend_kernel(*refs):
    arrived, (k1_ref, k2_ref, k3_ref, o_ref) = refs[:Z], refs[Z : Z + 4]
    attend_body(arrived, k1_ref, k2_ref, k3_ref, o_ref, *refs[Z + 4 :])


def attend_body(arrived, k1_ref, k2_ref, k3_ref, o_ref, kv_ref, qs_ref, tri_ref, carry_ref, acc_ref, steps_ref):
    here = lax.axis_index("x")
    plane = lax.axis_index("z")
    for i in range(Z):
        at = lax.rem(plane + (Z - i), Z)
        kv_ref[here, at] = arrived[i][HEAD:]
        for shift, piece in ((1, k1_ref), (2, k2_ref), (3, k3_ref)):
            kv_ref[lax.rem(here + (X - shift), X), at] = piece[i]
    row = lax.broadcasted_iota(jnp.int32, (256, 256), 0)
    col = lax.broadcasted_iota(jnp.int32, (256, 256), 1)
    tri_ref[...] = jnp.where(row > col, 1.0, 0.0).astype(BF)
    ones = jnp.where(lax.broadcasted_iota(jnp.int32, (64, 128), 0) == 0, 1.0, 0.0)
    for i in range(Z):
        q = jnp.concatenate([arrived[i][:HEAD].astype(F32), ones], axis=0)
        qs_ref[lax.rem(plane + (Z - i), Z)] = jnp.transpose(q).astype(BF)
    for i, step in enumerate(STEPS):
        for j, pair in enumerate(step):
            steps_ref[i, 2 * j] = pair[0]
            steps_ref[i, 2 * j + 1] = pair[1]

    def scores(b, t):
        keys = jnp.concatenate([kv_ref[i, t, 0:80, :] for i in range(4)], axis=1)
        return jnp.dot(qs_ref[b][:, 0:80], keys, preferred_element_type=F32)

    def tile(b, t, mask, carry):
        s = scores(b, t)
        sp = jnp.maximum(s, jnp.log(1.0 + jnp.exp(jnp.minimum(s, 80.0))))
        if mask is not None:
            sp = jnp.where(mask, sp, 0.0)
        rounded = sp.astype(BF)
        logit = s - sp
        weights = [None, None]
        for half in (1, 0):
            at = slice(half * 256, half * 256 + 256)
            behind = jnp.dot(rounded[:, at], tri_ref[...], preferred_element_type=F32)
            w = jnp.exp(logit[:, at] - behind - carry)
            if mask is not None:
                w = jnp.where(mask[:, at], w, 0.0)
            weights[half] = w.astype(BF)
            carry = carry + behind[:, 0:1] + sp[:, half * 256 : half * 256 + 1]
        values = jnp.concatenate([kv_ref[i, t, 80:144, :] for i in range(4)], axis=1)
        out = lax.dot_general(
            jnp.concatenate(weights, axis=1), values, (((1,), (1,)), ((), ())), preferred_element_type=F32
        )
        return out, carry

    def diagonal(i, unused):
        q_at = here * 128 + lax.broadcasted_iota(jnp.int32, (128, 512), 0)
        mask = lax.broadcasted_iota(jnp.int32, (128, 512), 1) < q_at
        done = [tile(j, j, mask, jnp.zeros((128, 1), F32)) for j in range(8)]
        for j in range(8):
            acc_ref[j] = done[j][0]
            carry_ref[j] = done[j][1]
        return unused

    lax.fori_loop(0, 1, diagonal, 0)

    def sweep(i, unused):
        blocks = [steps_ref[i, 2 * j] for j in range(4)]
        tiles = [steps_ref[i, 2 * j + 1] for j in range(4)]
        carries = [carry_ref[b] for b in blocks]
        before = [acc_ref[b] for b in blocks]
        done = [tile(blocks[j], tiles[j], None, carries[j]) for j in range(4)]
        for j in range(4):
            acc_ref[blocks[j]] = before[j] + done[j][0]
            carry_ref[blocks[j]] = done[j][1]
        return unused

    lax.fori_loop(0, len(STEPS), sweep, 0)
    for b in range(8):
        o_ref[b] = jnp.transpose(acc_ref[b]).astype(BF)


VMEM = pl.BlockSpec(memory_space=pltpu.VMEM)
ANY = pl.BlockSpec(memory_space=pl.ANY)


def attend(arrived, pieces):
    return pl.pallas_call(
        attend_kernel,
        out_shape=jax.ShapeDtypeStruct((8, HEAD, 128), BF),
        in_specs=[VMEM] * (Z + 3),
        out_specs=VMEM,
        scratch_shapes=[
            pltpu.VMEM((4, 8, 144, 128), BF),
            pltpu.VMEM((8, 128, 128), BF),
            pltpu.VMEM((256, 256), BF),
            pltpu.VMEM((8, 128, 1), F32),
            pltpu.VMEM((8, 128, HEAD), F32),
            pltpu.SMEM((len(STEPS), 8), jnp.int32),
        ],
        compiler_params=pltpu.CompilerParams(vmem_limit_bytes=14 * MIB),
        cost_estimate=pl.CostEstimate(flops=4_000_000_000, transcendentals=7_000_000, bytes_accessed=2_000_000),
    )(*arrived, *pieces)


def pack_kernel(q_ref, k_ref, v_ref, shift_ref, *refs):
    outs, (q_all, k_all, v_all, shift_all) = refs[:Z], refs[Z:]
    plane = lax.axis_index("z")
    q_all[...] = jnp.transpose(q_ref[...].astype(F32) * HEAD**-0.5)
    k_all[...] = jnp.transpose(k_ref[...].astype(F32))
    v_all[...] = jnp.transpose(v_ref[...].astype(F32))
    shift_all[...] = shift_ref[...].astype(F32)
    first = lax.broadcasted_iota(jnp.int32, (16, 128), 0) == 0
    for s, out in enumerate(outs):
        head = lax.rem(plane + s, Z)
        rows = pl.ds(pl.multiple_of(head * HEAD, HEAD), HEAD)
        out[0:64] = q_all[rows, :].astype(BF)
        out[64:128] = k_all[rows, :].astype(BF)
        shift = jnp.broadcast_to(shift_all[pl.ds(head, 1), :], (16, 128))
        out[128:144] = jnp.where(first, shift, 0.0).astype(BF)
        out[144:208] = v_all[rows, :].astype(BF)


def stack_kernel(*refs):
    for i in range(Z):
        refs[Z][i] = refs[i][HEAD:]


def stacked(arrived):
    return pl.pallas_call(
        stack_kernel,
        out_shape=jax.ShapeDtypeStruct((Z, 144, 128), BF),
        in_specs=[VMEM] * Z,
        out_specs=VMEM,
    )(*arrived)


def pack(queries, key_rows, value_rows, shift):
    rows, width = queries.shape
    return pl.pallas_call(
        pack_kernel,
        out_shape=[jax.ShapeDtypeStruct((208, 128), BF)] * Z,
        in_specs=[VMEM] * 4,
        out_specs=[VMEM] * Z,
        scratch_shapes=[pltpu.VMEM((width, rows), F32)] * 3 + [pltpu.VMEM((8, rows), F32)],
    )(queries, key_rows, value_rows, shift)


def shifted(value, axis, size, by):
    return lax.ppermute(value, axis, [(i, (i + by) % size) for i in range(size)])


def mixer(queries, key_rows, value_rows, key_shift, out_weight):
    heads = key_shift.shape[1]
    rows = queries.shape[0]
    packed = pack(queries, key_rows, value_rows, key_shift.T)
    arrived = [packed[0]] + [shifted(packed[by], "z", Z, by) for by in range(1, Z)]
    keys = stacked(arrived)
    pieces = [shifted(keys, "x", X, by) for by in (1, 2, 3)]
    out = attend(arrived, pieces)
    attended = lax.all_to_all(out, "z", split_axis=0, concat_axis=0, tiled=True)
    attended = attended.reshape(heads * HEAD, rows)
    partial = lax.dot_general(
        attended, out_weight, (((0,), (0,)), ((), ())), preferred_element_type=F32
    ).astype(BF)
    return summed_over_tp(partial)


def summed_over_tp(partial):
    y, core = lax.axis_index("y"), lax.axis_index("c")
    rows, width = partial.shape
    per = rows // (Y * C)
    parts = partial.reshape(Y, C, per, width)
    mine = lax.dynamic_index_in_dim(parts, core, 1, keepdims=False)
    other = lax.dynamic_index_in_dim(parts, 1 - core, 1, keepdims=False)
    both = (mine.astype(F32) + shifted(other, "c", C, 1).astype(F32)).astype(BF)
    total = lax.dynamic_index_in_dim(both, y, 0, keepdims=False).astype(F32)
    for by in (1, 2, 3):
        piece = lax.dynamic_index_in_dim(both, lax.rem(y + by, Y), 0, keepdims=False)
        total = total + shifted(piece, "y", Y, by).astype(F32)
    return total.astype(BF)


def selection(ids_ref, core):
    row = lax.broadcasted_iota(jnp.int32, (256, 128), 0)
    token = lax.broadcasted_iota(jnp.int32, (256, 128), 1)
    expert = lax.div(row, 8)
    named = [ids_ref[k : k + 1, :] == expert for k in range(2)]
    either = jnp.where(named[0] | named[1], 1.0, 0.0)
    before = lax.broadcasted_iota(jnp.int32, (128, 128), 0)
    after = lax.broadcasted_iota(jnp.int32, (128, 128), 1)
    earlier = jnp.where((before < after) & (lax.div(before, 16) == lax.div(after, 16)), 1.0, 0.0)
    slot = jnp.dot(either.astype(BF), earlier.astype(BF), preferred_element_type=F32)
    here = (lax.div(token, 16) == 2 * lax.div(lax.rem(row, 8), 2) + core) & (
        slot == lax.rem(row, 2).astype(F32)
    )
    return [jnp.where(n & here, 1.0, 0.0) for n in named]


def dispatch_kernel(ids_ref, rows_ref, out_ref, part_ref, sem):
    width = out_ref.shape[1]
    start = pl.multiple_of(lax.axis_index("y") * width, width)
    copy = pltpu.make_async_copy(rows_ref.at[:, pl.ds(start, width)], part_ref, sem)
    copy.start()
    first, second = selection(ids_ref, lax.axis_index("c"))
    pick = (first + second).astype(BF)
    copy.wait()
    out_ref[...] = jnp.dot(pick, part_ref[...], preferred_element_type=F32).astype(BF)


def dispatch(ids, rows):
    width = rows.shape[1] // Y
    return pl.pallas_call(
        dispatch_kernel,
        out_shape=jax.ShapeDtypeStruct((256, width), BF),
        in_specs=[VMEM, ANY],
        out_specs=VMEM,
        scratch_shapes=[pltpu.VMEM((128, width), BF), pltpu.SemaphoreType.DMA],
    )(ids, rows)


def collect_kernel(ids_ref, rows_ref, o0_ref, o1_ref, o2_ref, o3_ref, all_ref):
    y, core = lax.axis_index("y"), lax.axis_index("c")
    for k, pick in enumerate(selection(ids_ref, core)):
        chosen = jnp.transpose(pick).astype(BF)
        all_ref[k] = jnp.dot(chosen, rows_ref[...], preferred_element_type=F32).astype(BF)
        for s, out in enumerate((o0_ref, o1_ref, o2_ref, o3_ref)):
            at = pl.multiple_of((2 * lax.rem(y + s, Y) + core) * 16, 16)
            out[k] = all_ref[k, pl.ds(at, 16), :]


def collect(ids, rows):
    width = rows.shape[1]
    return pl.pallas_call(
        collect_kernel,
        out_shape=[jax.ShapeDtypeStruct((2, 16, width), BF)] * Y,
        in_specs=[VMEM, VMEM],
        out_specs=[VMEM] * Y,
        scratch_shapes=[pltpu.VMEM((2, 128, width), BF)],
        compiler_params=pltpu.CompilerParams(vmem_limit_bytes=5 * MIB),
    )(ids, rows)


def spread_kernel(weights_ref, out_ref):
    w = weights_ref[...]
    for k in range(2):
        out_ref[k] = jnp.broadcast_to(w[:, k : k + 1], (16, 128))


def spread_weights(weights):
    return pl.pallas_call(
        spread_kernel,
        out_shape=jax.ShapeDtypeStruct((2, 16, 128), F32),
        in_specs=[VMEM],
        out_specs=VMEM,
    )(weights)


def finish_kernel(p0_ref, p1_ref, p2_ref, p3_ref, weights_ref, out_ref):
    width = p0_ref.shape[2]
    w = [jnp.concatenate([weights_ref[k]] * (width // 128), axis=1) for k in range(2)]
    for s, p in enumerate((p0_ref, p1_ref, p2_ref, p3_ref)):
        at = pl.multiple_of(lax.rem(lax.axis_index("y") + (Y - s), Y) * width, width)
        total = p[0].astype(F32) * w[0] + p[1].astype(F32) * w[1]
        out_ref[:, pl.ds(at, width)] = total.astype(BF)


def finish(picked, weights):
    return pl.pallas_call(
        finish_kernel,
        out_shape=jax.ShapeDtypeStruct((16, Y * picked[0].shape[2]), BF),
        in_specs=[VMEM] * 5,
        out_specs=VMEM,
        compiler_params=pltpu.CompilerParams(vmem_limit_bytes=4 * MIB),
    )(*picked, weights)


def share_kernel(gate_ref, up_ref, down_ref, o0_ref, o1_ref, o2_ref, o3_ref, sem):
    width = gate_ref.shape[0] // Y
    copies = []
    for s, out in ((1, o1_ref), (2, o2_ref), (3, o3_ref), (0, o0_ref)):
        start = pl.multiple_of(lax.rem(lax.axis_index("y") + s, Y) * width, width)
        copies.append((gate_ref.at[pl.ds(start, width), :], out.at[pl.ds(0, width), :]))
        copies.append((up_ref.at[pl.ds(start, width), :], out.at[pl.ds(width, width), :]))
        for j in range(width // 128):
            copies.append(
                (
                    down_ref.at[:, pl.ds(pl.multiple_of(start + j * 128, 128), 128)],
                    out.at[pl.ds(2 * width + j * 128, 128), :],
                )
            )
    made = [pltpu.make_async_copy(a, b, sem.at[n]) for n, (a, b) in enumerate(copies)]
    for m in made:
        m.start()
    for m in made:
        m.wait()


def share(gate, up, down):
    width = gate.shape[0] // Y
    out = jax.ShapeDtypeStruct((3 * width, 128), BF)
    return pl.pallas_call(
        share_kernel,
        out_shape=[out] * Y,
        in_specs=[ANY, ANY, ANY],
        out_specs=[VMEM] * Y,
        scratch_shapes=[pltpu.SemaphoreType.DMA((Y * (2 + width // 128),))],
    )(gate, up, down)


def expand_kernel(*refs):
    rows_ref, ours, theirs, outs = refs[0], refs[1 : 1 + Y], refs[1 + Y : 1 + 2 * Y], refs[1 + 2 * Y :]
    width = rows_ref.shape[1]
    for s in (1, 2, 3, 0):
        parts = []
        for w_ref in (ours[s], theirs[s]):
            w = jnp.concatenate([w_ref[0:width], w_ref[width : 2 * width]], axis=1)
            parts.append(jnp.dot(rows_ref[...], w, preferred_element_type=F32))
        outs[s][...] = jnp.concatenate(parts, axis=1).astype(outs[s].dtype)


def expand(rows, ours, theirs):
    sent = jax.ShapeDtypeStruct((rows.shape[0], 512), BF)
    return pl.pallas_call(
        expand_kernel,
        out_shape=[jax.ShapeDtypeStruct((rows.shape[0], 512), F32), sent, sent, sent],
        in_specs=[VMEM] * (1 + 2 * Y),
        out_specs=[VMEM] * Y,
        compiler_params=pltpu.CompilerParams(vmem_limit_bytes=16 * MIB),
    )(rows, *ours, *theirs)


def hidden_kernel(p0_ref, p1_ref, p2_ref, p3_ref, o_ref):
    for n in range(C):
        both = p0_ref[:, n * 256 : n * 256 + 256]
        for p in (p1_ref, p2_ref, p3_ref):
            both = both + p[:, n * 256 : n * 256 + 256].astype(F32)
        gate, up = both[:, 0:128], both[:, 128:256]
        o_ref[:, n * 128 : n * 128 + 128] = (gate / (1.0 + jnp.exp(-gate)) * up).astype(BF)


def hidden_units(parts):
    return pl.pallas_call(
        hidden_kernel,
        out_shape=jax.ShapeDtypeStruct((parts[0].shape[0], 256), BF),
        in_specs=[VMEM] * 4,
        out_specs=VMEM,
        compiler_params=pltpu.CompilerParams(vmem_limit_bytes=5 * MIB),
    )(*parts)


def reduce_kernel(*refs):
    units, ours, theirs, o_ref = refs[:Y], refs[Y : 2 * Y], refs[2 * Y : 3 * Y], refs[3 * Y]
    width = o_ref.shape[1]
    columns = []
    for s in range(Y):
        for w_ref in (ours[s], theirs[s]):
            blocks = [w_ref[2 * width + j * 128 : 2 * width + j * 128 + 128] for j in range(width // 128)]
            columns.append(jnp.concatenate(blocks, axis=1))
    w = jnp.concatenate(columns, axis=0)
    h = jnp.concatenate([u[...] for u in units], axis=1)
    o_ref[...] = jnp.dot(h, w, preferred_element_type=F32).astype(BF)


def reduce_units(units, ours, theirs):
    rows = units[0].shape[0]
    width = ours[0].shape[0] // 3
    return pl.pallas_call(
        reduce_kernel,
        out_shape=jax.ShapeDtypeStruct((rows, width), BF),
        in_specs=[VMEM] * (3 * Y),
        out_specs=VMEM,
        compiler_params=pltpu.CompilerParams(vmem_limit_bytes=16 * MIB),
    )(*units, *ours, *theirs)


def experts(routed_rows, expert_ids, route_weights, gate_weight, up_weight, down_weight):
    ep = ("z", "x")
    ids = expert_ids.T
    width = routed_rows.shape[1] // Y
    kept = share(gate_weight[0], up_weight[0], down_weight[0])
    ours = [kept[0]] + [shifted(kept[s], "y", Y, s) for s in (1, 2, 3)]
    theirs = [shifted(w, "c", C, 1) for w in ours]
    outgoing = dispatch(ids, routed_rows).reshape(Z * X, 8, width)
    own = lax.all_to_all(outgoing, ep, split_axis=0, concat_axis=0, tiled=True).reshape(256, width)
    wide = spread_weights(route_weights)
    parts = expand(own, ours, theirs)
    summed = [parts[0]] + [shifted(parts[s], "y", Y, Y - s) for s in (1, 2, 3)]
    mine = hidden_units(summed)
    units = [mine] + [shifted(mine, "y", Y, s) for s in (1, 2, 3)]
    result = reduce_units(units, ours, theirs)
    returned = lax.all_to_all(
        result.reshape(Z * X, 8, width), ep, split_axis=0, concat_axis=0, tiled=True
    ).reshape(256, width)
    picked = collect(ids, returned)
    picked = [picked[0]] + [shifted(picked[s], "y", Y, s) for s in (1, 2, 3)]
    return finish(picked, wide)


def shards(
    queries,
    key_rows,
    value_rows,
    key_shift,
    out_weight,
    routed_rows,
    expert_ids,
    route_weights,
    gate_weight,
    up_weight,
    down_weight,
):
    mixed_rows = mixer(queries, key_rows, value_rows, key_shift, out_weight)
    routed_out = experts(routed_rows, expert_ids, route_weights, gate_weight, up_weight, down_weight)
    return (mixed_rows, routed_out)


def solution(mesh):
    mesh = Mesh(mesh.devices.reshape(Z, X, Y, C), ("z", "x", "y", "c"))
    ep, tp = ("z", "x"), ("y", "c")
    return jax.shard_map(
        shards,
        mesh=mesh,
        in_specs=(
            P(ep, tp),
            P(ep, tp),
            P(ep, tp),
            P(ep, tp),
            P(tp, None),
            P(ep, None),
            P(ep, None),
            P(ep + tp, None),
            P(ep, None, tp),
            P(ep, None, tp),
            P(ep, tp, None),
        ),
        out_specs=(P(ep + tp, None), P(ep + tp, None)),
        check_vma=False,
    )
```
